256 devices in a mesh: ep: 16 (over y, x), tp: 16 (over z, core).
Axes of the slice: x: 4, y: 4, z: 8, core: 2. Of those that a mesh axis runs over, the one named last changes fastest.
Arguments:
- tokens: bfloat16 [256, 4096], P('ep'), may hold values from -6 to 6
- query_weight: bfloat16 [4096, 4096], P('ep', 'tp'), may hold values from -0.09375 to 0.09375
- key_weight: bfloat16 [4096, 2048], P('ep', 'tp'), may hold values from -0.15625 to 0.15625
- value_weight: bfloat16 [4096, 2048], P('ep', 'tp'), may hold values from -0.09375 to 0.09375
- out_weight: bfloat16 [4096, 4096], P('tp', 'ep'), may hold values from -0.09375 to 0.09375
- head_lambda: float32 [32], P('tp'), may hold values from 0.3 to 0.8
- head_gain: float32 [128], replicated, may hold values from 0.1 to 1.9
- key_cache: bfloat16 [256, 1024, 16, 128], P('ep', None, 'tp'), may hold values from -1000 to 1000
- value_cache: bfloat16 [256, 1024, 16, 128], P('ep', None, 'tp'), may hold values from -6 to 6
- lengths: int32 [256], P('ep'), may hold values from 128 to 1024, as said below
- first_gain: float32 [4096], replicated, may hold values from 0.3 to 3
- second_gain: float32 [4096], P('tp'), may hold values from 0.1 to 1.9
- expert_ids: int32 [256, 2], P('ep'), may hold values from 0 to 15, all different within a row; in each aligned block of 16 rows (0 to 15, 16 to 31, ...) at most 4 rows name the same one
- route_weights: float32 [256, 2], P('ep'), may hold values from 0.1 to 1
- expert_gate: bfloat16 [16, 4096, 2048], P('ep', 'tp'), may hold values from -0.09375 to 0.09375
- expert_up: bfloat16 [16, 4096, 2048], P('ep', 'tp'), may hold values from -0.09375 to 0.09375
- expert_down: bfloat16 [16, 2048, 4096], P('ep', None, 'tp'), may hold values from -0.125 to 0.125
- dense_gate: bfloat16 [4096, 2048], P('tp', 'ep'), may hold values from -0.09375 to 0.09375
- dense_up: bfloat16 [4096, 2048], P('tp', 'ep'), may hold values from -0.09375 to 0.09375
- dense_down: bfloat16 [2048, 4096], P('ep', 'tp'), may hold values from -0.25 to 0.25
- dense_mix: bfloat16 [4096], replicated, may hold values from -0.09375 to 0.09375
Outputs:
- layer_out: bfloat16 [256, 4096], P('ep', 'tp')
The draws below stay inside these ranges and needn't reach their ends.
Inputs may be any that keep to these rules, and one draw needn't show every extreme that they name: `lengths`: positions below a sequence's length hold its cache; the new token stands at that position. Some sequence has length 1024 in every draw. `expert_ids`: each row names 2 different experts. Among the rows of one device's 16 sequences (aligned blocks) no expert is named more than 4 times, and in every draw some expert is named exactly 4 times in some block.
All inputs are finite; a program needn't handle non-finite values.
Results may differ from the reference program's by a relative error of at most 0.04.
Values may be sent and summed in bfloat16 or wider, within the bound.
A program may use at most 64 MiB of HBM per device.

```python
import math
import jax
import jax.numpy as jnp
import numpy as np
from jax import lax

D = 4096
HEADS = 32
KV_HEADS = 16
SUB = 64
VD = 128
EXPERTS = 16
FFE = 2048
FFD = 2048
TOPK = 2
SEQ_DEV = 16
CACHE = 1024
SEQS = 256
CAP = 4


def draw_key_cache(key, part):
    rand_keys = jax.random.split(jax.random.fold_in(key, 11), 1)
    full_shape = (SEQS, CACHE, KV_HEADS, 2 * SUB)
    values = jnp.clip(1.75 * jax.random.normal(rand_keys[0], full_shape, jnp.float32), -10.5, 10.5)
    return values.astype(jnp.bfloat16)


def draw_lengths(key, part):
    rand_keys = jax.random.split(jax.random.fold_in(key, 23), 3)
    group_rate = jax.random.randint(rand_keys[0], (SEQS // SEQ_DEV,), 1, 5)
    seq_rate = jnp.repeat(group_rate, SEQ_DEV)
    shortest = CACHE // 8
    raw_draw = jax.random.randint(rand_keys[1], (SEQS,), 0, CACHE)
    lengths = shortest + raw_draw * seq_rate * (CACHE - shortest) // (4 * CACHE)
    longest = jax.random.randint(rand_keys[2], (), 0, SEQS)
    return jnp.where(jnp.arange(SEQS, dtype=jnp.int32) == longest, CACHE, lengths).astype(jnp.int32)


def draw_first_gain(key, part):
    rand_keys = jax.random.split(jax.random.fold_in(key, 37), 2)
    ramp = jnp.arange(D, dtype=jnp.float32) / (D - 1)
    trend = jnp.exp(jnp.log(0.5) + ramp * (jnp.log(2.0) - jnp.log(0.5)))
    rough = jax.random.uniform(rand_keys[1], (D,), jnp.float32, 0.7, 1.4)
    return (trend * rough).astype(jnp.float32)


def steps_of(key, dims, cuts, least, top_value):
    factor_of = 1.0
    for dim, parts in cuts:
        steps = jax.random.uniform(jax.random.fold_in(jax.random.fold_in(key, 6), dim), (parts,), jnp.float32, least / len(cuts), top_value / len(cuts))
        factor_of = factor_of * jnp.repeat(jnp.exp(steps), dims[dim] // parts).reshape((-1,) + (1,) * (len(dims) - 1 - dim))
    return factor_of


def assign_block(own_key, own, number, rows, count, top, limit, skew):
    ranking = jax.random.permutation(own_key, count)
    heavy_load, usual = portions_of(count, rows * top, limit, skew, True), portions_of(count, rows * top, limit, skew, False)
    places = jnp.arange(count)

    def named(sizes, rotation):
        used = int((sizes > 0).sum())
        fixed = max(1, used // 4)
        passed = fixed + (places - fixed + rotation * (used - fixed)) % max(1, count - fixed)
        return jnp.zeros((count,), jnp.int32).at[ranking[jnp.where(places < fixed, places, passed)]].set(jnp.asarray(sizes, jnp.int32))

    sizes = jnp.where(number % 4 == 0, named(heavy_load, number // 4), named(usual, number - number // 4 - 1))
    mixed = jax.random.permutation(jax.random.fold_in(own, 3), count)
    giver, sink = mixed[0:count // 2 * 2:2], mixed[1:count // 2 * 2:2]
    slack = jnp.minimum(sizes[giver] - 1, limit - sizes[sink]) // 2
    slack = jnp.where((giver == ranking[0]) | (sink == ranking[0]) | (sizes[sink] == 0), 0, jnp.maximum(slack, 0))
    passed = jax.random.randint(jax.random.fold_in(own, 4), (count // 2,), 0, 1 << 20) % (slack + 1)
    sizes = sizes.at[giver].add(-passed).at[sink].add(passed)
    items = jnp.searchsorted(jnp.cumsum(sizes), jnp.arange(rows * top), side="right").astype(jnp.int32)
    table = items.reshape(top, rows).T
    table = table[jax.random.permutation(jax.random.fold_in(own, 1), rows)]
    rotation = jax.random.randint(jax.random.fold_in(own, 2), (rows, 1), 0, top)
    return jnp.take_along_axis(table, (jnp.arange(top)[None, :] + rotation) % top, axis=1)


def portions_of(amount, total, bound, lean, full):
    portions = [(1 << 20) // math.isqrt(rank ** lean) + 1 for rank in range(1, amount + 1)]
    largest = bound if full else min(bound, max(-(-total // amount), total * portions[0] // sum(portions)))
    least = 1 if total - largest >= amount - 1 else 0
    given, rest = [largest] + [least] * (amount - 1), total - largest - least * (amount - 1)
    while rest > 0:
        movable = [i for i in range(1, amount) if given[i] < largest] or [i for i in range(1, amount) if given[i] < bound]
        mass, left = sum([portions[i] for i in movable]), rest
        for i in movable:
            addition = min(bound - given[i], max(1, left * portions[i] // mass), rest)
            given[i] = given[i] + addition
            rest = rest - addition
    return np.array(given)


def centred(rng, shape, scale, bound, cuts=(), kind=jnp.bfloat16):
    drawn = scale * jax.random.normal(rng, shape, jnp.float32)
    if cuts:
        drawn = drawn * steps_of(rng, shape, cuts, -0.22, 0.18)
    return jnp.clip(drawn, -bound, bound).astype(kind)


def setup_inputs(seed: int = 0) -> dict:
    splits = jax.random.split(jax.random.key(seed), 22)
    tokens = centred(splits[0], (SEQS, D), 1.0, 6.0, ((0, 16),))
    query_weight = centred(splits[1], (D, HEADS * 2 * SUB), D ** -0.5, 0.09375, ((0, 16), (1, 16)))
    key_weight = centred(splits[2], (D, KV_HEADS * 2 * SUB), (D // 3) ** -0.5, 0.15625, ((0, 16), (1, 16)))
    value_weight = centred(splits[3], (D, KV_HEADS * VD), D ** -0.5, 0.09375, ((0, 16), (1, 16)))
    out_weight = centred(splits[4], (HEADS * VD, D), (HEADS * VD) ** -0.5, 0.09375, ((0, 16), (1, 16)))
    head_lambda = jnp.clip(0.3 + 0.5 * jax.random.uniform(splits[5], (HEADS,), jnp.float32) ** steps_of(splits[5], (HEADS,), ((0, 16),), -0.2, 0.2), 0.3, 0.8)
    head_gain = jnp.clip(1.0 + 0.18 * jax.random.normal(splits[6], (VD,), jnp.float32), 0.1, 1.9)
    key_cache = draw_key_cache(jax.random.fold_in(splits[21], 71), 0)
    value_cache = centred(splits[8], (SEQS, CACHE, KV_HEADS, VD), 1.0, 6.0, ((0, 16), (2, 16)))
    lengths = draw_lengths(jax.random.fold_in(splits[21], 71), 0)
    first_gain = draw_first_gain(jax.random.fold_in(splits[21], 71), 0)
    second_gain = jnp.clip(1.0 + 0.18 * jax.random.normal(splits[11], (D,), jnp.float32), 0.1, 1.9)
    expert_ids_keys = jax.random.split(jax.random.fold_in(splits[12], 1), SEQS // SEQ_DEV)
    expert_ids_turns = jax.random.permutation(jax.random.fold_in(splits[12], 3), SEQS // SEQ_DEV)
    expert_ids = jax.vmap(lambda own, number: assign_block(jax.random.fold_in(splits[12], 2), own, number, SEQ_DEV, EXPERTS, TOPK, CAP, 2))(expert_ids_keys, expert_ids_turns).reshape((SEQS, TOPK))
    route_weights = jnp.clip(jnp.exp(math.log(1.0) - 2.3025851 * jax.random.uniform(splits[13], (SEQS, TOPK), jnp.float32) ** steps_of(splits[13], (SEQS, TOPK), ((0, 16),), -0.2, 0.2)), 0.1, 1.0)
    expert_gate = centred(splits[14], (EXPERTS, D, FFE), D ** -0.5, 0.09375, ((0, 16), (1, 16)))
    expert_up = centred(splits[15], (EXPERTS, D, FFE), D ** -0.5, 0.09375, ((0, 16), (1, 16)))
    expert_down = centred(splits[16], (EXPERTS, FFE, D), FFE ** -0.5, 0.125, ((0, 16), (2, 16)))
    dense_gate = centred(splits[17], (D, FFD), D ** -0.5, 0.09375, ((0, 16), (1, 16)))
    dense_up = centred(splits[18], (D, FFD), D ** -0.5, 0.09375, ((0, 16), (1, 16)))
    dense_down = centred(splits[19], (FFD, D), (FFD // 4) ** -0.5, 0.25, ((0, 16), (1, 16)))
    dense_mix = centred(splits[20], (D,), D ** -0.5, 0.09375)
    return dict(tokens=tokens, query_weight=query_weight, key_weight=key_weight, value_weight=value_weight, out_weight=out_weight, head_lambda=head_lambda, head_gain=head_gain, key_cache=key_cache, value_cache=value_cache, lengths=lengths, first_gain=first_gain, second_gain=second_gain, expert_ids=expert_ids, route_weights=route_weights, expert_gate=expert_gate, expert_up=expert_up, expert_down=expert_down, dense_gate=dense_gate, dense_up=dense_up, dense_down=dense_down, dense_mix=dense_mix)


theta_base = 500000.0
score_scale = 0.125
head_scale = 0.8
residual_scale = 2.0 ** 0.5
layer_epsilon = 1e-05
head_epsilon = 1e-06

def rotate(vector, cosine, sine_table):
    middle = vector.shape[-1] // 2
    lower = vector[..., :middle]
    upper = vector[..., middle:]
    return jnp.concatenate([lower * cosine - upper * sine_table, upper * cosine + lower * sine_table], axis=-1)

def rounded(array):
    return lax.optimization_barrier(array.astype(jnp.bfloat16)).astype(jnp.float32)

def reference(tokens, query_weight, key_weight, value_weight, out_weight, head_lambda, head_gain, key_cache, value_cache, lengths, first_gain, second_gain, expert_ids, route_weights, expert_gate, expert_up, expert_down, dense_gate, dense_up, dense_down, dense_mix):
    group_size = HEADS // KV_HEADS
    frequency = theta_base ** (-(jnp.arange(SUB // 2, dtype=jnp.float32) * (2.0 / SUB)))
    angles = lengths.astype(jnp.float32)[:, None] * frequency[None, :]
    cosine = jnp.cos(angles)
    sine_table = jnp.sin(angles)
    query_rows = rounded(jnp.dot(tokens, query_weight, preferred_element_type=jnp.float32))
    query_rows = query_rows.reshape(SEQS, KV_HEADS, group_size, 2, SUB)
    query_rows = rounded(rotate(query_rows, cosine[:, None, None, None, :], sine_table[:, None, None, None, :]))
    new_keys = rounded(jnp.dot(tokens, key_weight, preferred_element_type=jnp.float32))
    new_keys = rounded(rotate(new_keys.reshape(SEQS, KV_HEADS, 2, SUB), cosine[:, None, None, :], sine_table[:, None, None, :]))
    new_values = rounded(jnp.dot(tokens, value_weight, preferred_element_type=jnp.float32))
    new_values = new_values.reshape(SEQS, KV_HEADS, VD)
    lambdas = head_lambda.reshape(KV_HEADS, group_size)
    valid = jnp.arange(CACHE, dtype=jnp.int32)[None, :] < lengths[:, None]

    def head_step(head):
        cached_keys = lax.dynamic_index_in_dim(key_cache, head, 2, keepdims=False).astype(jnp.float32)
        cached_keys = cached_keys.reshape(SEQS, CACHE, 2, SUB)
        cached_values = lax.dynamic_index_in_dim(value_cache, head, 2, keepdims=False).astype(jnp.float32)
        head_query = lax.dynamic_index_in_dim(query_rows, head, 1, keepdims=False)
        head_key = lax.dynamic_index_in_dim(new_keys, head, 1, keepdims=False)
        head_value = lax.dynamic_index_in_dim(new_values, head, 1, keepdims=False)
        pair = lax.dynamic_index_in_dim(lambdas, head, 0, keepdims=False)
        scores = jnp.einsum('sgcd,sjcd->sgcj', head_query, cached_keys) * score_scale
        scores = jnp.where(valid[:, None, None, :], scores, -jnp.inf)
        fresh_score = jnp.einsum('sgcd,scd->sgc', head_query, head_key) * score_scale
        highest = jnp.maximum(lax.optimization_barrier(jnp.max(scores, axis=-1)), fresh_score)
        cached_exp = jnp.exp(scores - highest[..., None])
        fresh_exp = jnp.exp(fresh_score - highest)
        denominator = lax.optimization_barrier(jnp.sum(cached_exp, axis=-1)) + fresh_exp
        cached_prob = cached_exp / denominator[..., None]
        fresh_prob = fresh_exp / denominator
        mixed_map = rounded(cached_prob[:, :, 0] - pair[None, :, None] * cached_prob[:, :, 1])
        mixed_new = rounded(fresh_prob[:, :, 0] - pair[None, :] * fresh_prob[:, :, 1])
        return jnp.einsum('sgj,sje->sge', mixed_map, cached_values) + mixed_new[..., None] * head_value[:, None, :]
    head_out = lax.map(head_step, jnp.arange(KV_HEADS, dtype=jnp.int32))
    head_out = jnp.moveaxis(head_out, 0, 1)
    square_mean = lax.optimization_barrier(jnp.mean(head_out * head_out, axis=-1, keepdims=True))
    normed = head_out * lax.rsqrt(square_mean + head_epsilon) * head_gain * head_scale
    normed = normed.astype(jnp.bfloat16).reshape(SEQS, HEADS * VD)
    attention = rounded(jnp.dot(normed, out_weight, preferred_element_type=jnp.float32))
    residual_in = residual_scale * tokens.astype(jnp.float32) + attention
    average = lax.optimization_barrier(jnp.mean(residual_in, axis=-1, keepdims=True))
    centered = residual_in - average
    variance = lax.optimization_barrier(jnp.mean(centered * centered, axis=-1, keepdims=True))
    hidden_in = (centered * lax.rsqrt(variance + layer_epsilon) * first_gain).astype(jnp.bfloat16)
    route_gates = route_weights / lax.optimization_barrier(jnp.sum(route_weights, axis=-1, keepdims=True))

    def expert_step(running, expert):
        gate_matrix = lax.dynamic_index_in_dim(expert_gate, expert, 0, keepdims=False)
        up_matrix = lax.dynamic_index_in_dim(expert_up, expert, 0, keepdims=False)
        down_matrix = lax.dynamic_index_in_dim(expert_down, expert, 0, keepdims=False)
        pre_gate = jnp.dot(hidden_in, gate_matrix, preferred_element_type=jnp.float32)
        pre_up = jnp.dot(hidden_in, up_matrix, preferred_element_type=jnp.float32)
        expert_hidden = (jax.nn.silu(pre_gate) * pre_up).astype(jnp.bfloat16)
        expert_result = rounded(jnp.dot(expert_hidden, down_matrix, preferred_element_type=jnp.float32))
        token_weight = lax.optimization_barrier(jnp.sum(jnp.where(expert_ids == expert, route_gates, 0.0), axis=-1))
        return (running + token_weight[:, None] * expert_result, None)
    expert_mix, _ = lax.scan(expert_step, jnp.zeros((SEQS, D), jnp.float32), jnp.arange(EXPERTS, dtype=jnp.int32))
    dense_pre_gate = jnp.dot(hidden_in, dense_gate, preferred_element_type=jnp.float32)
    dense_pre_up = jnp.dot(hidden_in, dense_up, preferred_element_type=jnp.float32)
    dense_hidden = (jax.nn.silu(dense_pre_gate) * dense_pre_up).astype(jnp.bfloat16)
    dense_out = rounded(jnp.dot(dense_hidden, dense_down, preferred_element_type=jnp.float32))
    mix_gate = jax.nn.sigmoid(jnp.dot(hidden_in, dense_mix, preferred_element_type=jnp.float32))
    combined = residual_scale * hidden_in.astype(jnp.float32) + expert_mix + mix_gate[:, None] * dense_out
    average = lax.optimization_barrier(jnp.mean(combined, axis=-1, keepdims=True))
    variance = lax.optimization_barrier(jnp.mean(combined * combined, axis=-1, keepdims=True)) - average * average
    return ((combined - average) * lax.rsqrt(variance + layer_epsilon) * second_gain).astype(jnp.bfloat16)
```

```python
import functools
import math

import jax
import jax.numpy as jnp
from jax import lax
from jax.experimental import pallas as pl
from jax.experimental.pallas import tpu as pltpu
from jax.sharding import PartitionSpec as P

N = 16
CACHE = 1024
CAP = 4
F32 = jnp.float32
BF16 = jnp.bfloat16
MESH = pl.DeviceIdType.MESH

PA, PMETA, PB, PD, PE, PF, PG, PMIX, PH, PI, PI2, PJ, PK = range(13)
PHASES = 13

LOCALS = (
    "tok", "qw", "kw", "vw", "ow", "lam", "hgain", "kc", "vc", "lens", "fgain",
    "sgain", "ids", "rw", "eg", "eu", "ed", "dg", "du", "dd", "dmix",
)


def dot(a, b):
    return jnp.dot(a, b, preferred_element_type=F32)


def to_column(row, n):
    same = lax.broadcasted_iota(jnp.int32, (n, n), 0) == lax.broadcasted_iota(jnp.int32, (n, n), 1)
    return jnp.sum(jnp.where(same, jnp.broadcast_to(row, (n, n)), 0), axis=1, keepdims=True)


def to_row(column, n, lanes):
    same = lax.broadcasted_iota(jnp.int32, (n, lanes), 0) == lax.broadcasted_iota(
        jnp.int32, (n, lanes), 1
    )
    return jnp.sum(jnp.where(same, jnp.broadcast_to(column, (n, lanes)), 0), axis=0, keepdims=True)


def kernel(
    tok_h, qw_h, kw_h, vw_h, ow_h, lam_h, hgain_h, kc_h, vc_h, lens_h, fgain_h, sgain_h,
    ids_h, rw_h, eg_h, eu_h, ed_h, dg_h, du_h, dd_h, dmix_h,
    out_ref,
    tok, wqkv, ow, lam, hgain, kc, vc, lens, fgain, sgain, ids, rw, wgu, ed, wd, dd, dmix,
    xcol, meta, metas, bsend, brecv, qs, kn, vn, h0, h1, lens_b, dsend, drecv, esend, erecv,
    fsend, frecv, gsend, grecv, msend, mrecv, gw, hsend, hrecv, isend, isend2, ihid, idense,
    jsend, jrecv, ksend, krecv, pick, place, gates,
    lsem, ssem, rsem, ready,
):
    e = lax.axis_index("ep")
    t = lax.axis_index("tp")

    def chunk(i, width):
        return pl.ds(pl.multiple_of(i * width, width), width)

    def bring(name, pairs):
        sem = lsem.at[LOCALS.index(name)]
        for src, dst in pairs:
            pltpu.make_async_copy(src, dst, sem).start()

    def arrived(name, whole):
        pltpu.make_async_copy(whole, whole, lsem.at[LOCALS.index(name)]).wait()

    bring("tok", [(tok_h, tok)])
    bring("ids", [(ids_h, ids)])
    bring("rw", [(rw_h, rw)])
    bring("qw", [(qw_h, wqkv.at[:, 0:256])])
    bring("kw", [(kw_h, wqkv.at[:, 256:384])])
    bring("vw", [(vw_h, wqkv.at[:, 384:512])])
    bring("lens", [(lens_h, lens)])
    bring("lam", [(lam_h, lam)])
    bring("hgain", [(hgain_h, hgain)])
    bring("kc", [(kc_h, kc)])
    bring("vc", [(vc_h, vc)])
    bring("ow", [(ow_h, ow)])
    bring("fgain", [(fgain_h, fgain)])
    bring("dmix", [(dmix_h, dmix)])
    bring("sgain", [(sgain_h, sgain)])

    def bring_pair(i, _):
        sem_g = lsem.at[LOCALS.index("eg")]
        sem_u = lsem.at[LOCALS.index("eu")]
        even = pl.ds(pl.multiple_of(i * 256, 256), 128)
        odd = pl.ds(pl.multiple_of(i * 256 + 128, 128), 128)
        pltpu.make_async_copy(eg_h.at[:, chunk(i, 128)], wgu.at[:, even], sem_g).start()
        pltpu.make_async_copy(eu_h.at[:, chunk(i, 128)], wgu.at[:, odd], sem_u).start()
        return 0

    lax.fori_loop(0, N, bring_pair, 0)
    bring("dg", [(dg_h, wd.at[:, 0:128])])
    bring("du", [(du_h, wd.at[:, 128:256])])
    bring("ed", [(ed_h, ed)])
    bring("dd", [(dd_h, dd)])

    barrier = pltpu.get_barrier_semaphore()

    def greet(k, _):
        pl.semaphore_signal(
            barrier, inc=1, device_id=(lax.rem(e + k, N), t), device_id_type=MESH
        )
        pl.semaphore_signal(
            barrier, inc=1, device_id=(e, lax.rem(t + k, N)), device_id_type=MESH
        )
        return 0

    lax.fori_loop(1, N, greet, 0)

    def send(phase, src, dst, to):
        pltpu.make_async_remote_copy(
            src_ref=src,
            dst_ref=dst,
            send_sem=ssem.at[phase],
            recv_sem=rsem.at[phase],
            device_id=to,
            device_id_type=MESH,
        ).start()

    def over_ep(phase, src_of, dst):
        def one(k, _):
            a = lax.rem(e + k, N)
            send(phase, src_of(a), dst, (a, t))
            return 0

        lax.fori_loop(1, N, one, 0)

    def over_tp(phase, src_of, dst):
        def one(k, _):
            b = lax.rem(t + k, N)
            send(phase, src_of(b), dst, (e, b))
            return 0

        lax.fori_loop(1, N, one, 0)

    def received(phase, blocks):
        pltpu.make_async_copy(blocks, blocks, rsem.at[phase]).wait()

    def sent(phase, blocks):
        pltpu.make_async_copy(blocks, blocks, ssem.at[phase]).wait()

    lane = lax.broadcasted_iota(jnp.int32, (N, 128), 1)

    arrived("ids", ids)
    arrived("rw", rw)
    id0 = to_column(ids[0:1, :], N)
    id1 = to_column(ids[1:2, :], N)
    w0 = to_column(rw[0:1, :], N)
    w1 = to_column(rw[1:2, :], N)
    total = w0 + w1
    hit0 = lane == id0
    hit1 = lane == id1
    hit = jnp.where(hit0 | hit1, 1.0, 0.0).astype(F32)
    before = jnp.where(
        lax.broadcasted_iota(jnp.int32, (N, N), 1) < lax.broadcasted_iota(jnp.int32, (N, N), 0),
        1.0,
        0.0,
    ).astype(F32)
    slot = dot(before.astype(BF16), hit.astype(BF16))
    code = jnp.where(hit > 0.5, slot, -1.0)
    gate0 = jnp.where(lane - N == id0, w0 / total, 0.0)
    gate1 = jnp.where(lane - N == id1, w1 / total, 0.0)
    meta[...] = jnp.where(lane < N, code, gate0 + gate1)
    metas[e] = meta[...]

    arrived("tok", tok)
    xcol[e] = tok[:, chunk(e, 256)]

    pl.semaphore_wait(barrier, 2 * (N - 1))

    over_ep(PA, lambda a: tok.at[:, chunk(a, 256)], xcol.at[e])
    over_ep(PMETA, lambda a: meta, metas.at[e])

    def tell(k, _):
        pl.semaphore_signal(ready, inc=1, device_id=(e, lax.rem(t + k, N)), device_id_type=MESH)
        return 0

    lax.fori_loop(1, N, tell, 0)

    arrived("lens", lens)
    length = to_column(lens[...], N)
    lens_b[...] = jnp.broadcast_to(length, (N, 128))
    turn = lax.rem(lane, 32).astype(F32) * (2.0 / 64)
    angle = length.astype(F32) * jnp.exp(turn * (-math.log(500000.0)))
    low = lax.rem(lane, 64) < 32
    cosine = jnp.cos(angle)
    sine = jnp.sin(angle)
    sine = jnp.where(low, -sine, sine)

    arrived("qw", wqkv.at[:, 0:256])
    arrived("kw", wqkv.at[:, 256:384])
    arrived("vw", wqkv.at[:, 384:512])
    received(PA, xcol.at[0:15])
    bsend[...] = dot(xcol[...].reshape(256, 256), wqkv[...]).astype(BF16).reshape(N, N, 512)
    brecv[e] = bsend[e]
    over_ep(PB, lambda a: bsend.at[a], brecv.at[e])

    received(PMETA, metas.at[0:15])
    every = metas[...].reshape(256, 128)
    wide_lane = lax.broadcasted_iota(jnp.int32, (256, 128), 1)
    code_col = jnp.sum(jnp.where(wide_lane == e, every, 0.0), axis=1, keepdims=True)
    gate_col = jnp.sum(jnp.where(wide_lane == e + N, every, 0.0), axis=1, keepdims=True)
    block = (lax.broadcasted_iota(jnp.int32, (256, 1), 0) // N * CAP).astype(F32)
    target = jnp.where(code_col >= 0.0, code_col + block, -1.0)
    place[...] = jnp.where(
        lax.broadcasted_iota(jnp.int32, (256, 64), 1).astype(F32) == target, 1.0, 0.0
    ).astype(BF16)
    pick[...] = jnp.where(
        lax.broadcasted_iota(jnp.int32, (64, 256), 0).astype(F32) == to_row(target, 256, 256),
        1.0,
        0.0,
    ).astype(BF16)
    gates[...] = gate_col

    received(PB, brecv.at[0:15])
    qkv = jnp.sum(brecv[...].astype(F32), axis=0).astype(BF16).astype(F32)

    def rotated(x):
        swapped = jnp.where(low, pltpu.roll(x, 96, 1), pltpu.roll(x, 32, 1))
        return (x * cosine + swapped * sine).astype(BF16).astype(F32)

    first = lane < 64
    qs[...] = jnp.zeros_like(qs)
    for g in range(2):
        q = rotated(qkv[:, g * 128 : (g + 1) * 128]) * 0.125
        qs[pl.ds(g, N, stride=8), :] = jnp.where(first, q, 0.0)
        qs[pl.ds(g + 4, N, stride=8), :] = jnp.where(first, 0.0, q)
    kn[...] = rotated(qkv[:, 256:384])
    vn[...] = qkv[:, 384:512]

    arrived("lam", lam)
    row8 = lax.broadcasted_iota(jnp.int32, (8, 1), 0)
    share = jnp.where(row8 == 4, -lam[0:1, 0:1], jnp.where(row8 == 5, -lam[0:1, 1:2], 1.0))
    place_of = lax.broadcasted_iota(jnp.int32, (8, CACHE), 1)

    arrived("kc", kc)
    arrived("vc", vc)

    def attend(s):
        q = qs[pl.ds(pl.multiple_of(s * 8, 8), 8), :]
        scores = lax.dot_general(
            q.astype(BF16), kc[s], (((1,), (1,)), ((), ())), preferred_element_type=F32
        )
        fresh = jnp.sum(q * kn[pl.ds(s, 1), :], axis=1, keepdims=True)
        scores = jnp.where(place_of < lens_b[pl.ds(s, 1), 0:1], scores, -1e30)
        top = jnp.maximum(jnp.max(scores, axis=1, keepdims=True), fresh)
        p = jnp.exp(scores - top)
        fresh_p = jnp.exp(fresh - top)
        scale = share / (jnp.sum(p, axis=1, keepdims=True) + fresh_p)
        p = p * scale
        fresh_p = fresh_p * scale
        p = p + pltpu.roll(p, 4, 0)
        fresh_p = jnp.broadcast_to(fresh_p, (8, 128))
        fresh_p = (fresh_p + pltpu.roll(fresh_p, 4, 0)).astype(BF16).astype(F32)
        head = dot(p.astype(BF16), vc[s]) + fresh_p * vn[pl.ds(s, 1), :]
        h0[pl.ds(s, 1), :] = head[0:1, :]
        h1[pl.ds(s, 1), :] = head[1:2, :]

    def attend_some(i, _):
        for j in range(4):
            attend(i * 4 + j)
        return 0

    lax.fori_loop(0, N // 4, attend_some, 0)

    arrived("hgain", hgain)
    for g, ref in enumerate((h0, h1)):
        head = ref[...]
        mean = jnp.mean(head * head, axis=1, keepdims=True)
        head = head * lax.rsqrt(mean + 1e-6) * hgain[...] * 0.8
        dsend[:, g * 128 : (g + 1) * 128] = head.astype(BF16)
    drecv[e] = dsend[...]
    over_ep(PD, lambda a: dsend, drecv.at[e])

    arrived("ow", ow)
    arrived("fgain", fgain)
    arrived("dmix", dmix)
    gw[...] = fgain[...] * dmix[...].astype(F32)

    def block_of(ref):
        return jnp.concatenate([ref[pl.ds(2 * t, 1), :], ref[pl.ds(2 * t + 1, 1), :]], axis=1)

    gain = block_of(fgain)
    gain_mix = block_of(gw)
    pl.semaphore_wait(ready, N - 1)
    received(PD, drecv.at[0:15])
    esend[...] = dot(drecv[...].reshape(256, 256), ow[...]).astype(BF16).reshape(N, N, 256)

    def spread(k, _):
        a = lax.rem(e + k, N)
        send(PE, esend.at[a], erecv.at[t], (a, e))
        return 0

    lax.fori_loop(1, N, spread, 0)

    @pl.when(e == t)
    def _():
        pltpu.make_async_copy(esend.at[e], erecv.at[t], rsem.at[PE]).start()

    @pl.when(e != t)
    def _():
        send(PE, esend.at[e], erecv.at[t], (e, e))

    received(PE, erecv)
    root = 2.0**0.5
    attention = jnp.sum(erecv[...].astype(F32), axis=0).astype(BF16).astype(F32)
    residual = root * tok[:, chunk(t, 256)].astype(F32) + attention

    def block_moments(x):
        mean = jnp.sum(x, axis=1, keepdims=True) * (1.0 / 256)
        centred = x - mean
        return mean, centred, jnp.sum(centred * centred, axis=1, keepdims=True)

    mean_b, centred, square_b = block_moments(residual)
    mixed_b = jnp.sum(centred * gain_mix, axis=1, keepdims=True)
    gain_b = jnp.sum(gain_mix, axis=1, keepdims=True)
    fsend[0:1, :] = to_row(mean_b, N, 128)
    fsend[1:2, :] = to_row(square_b, N, 128)
    fsend[2:3, :] = to_row(mixed_b, N, 128)
    fsend[3:4, :] = jnp.broadcast_to(gain_b, (1, 128))
    frecv[t] = fsend[...]
    over_tp(PF, lambda b: fsend, frecv.at[t])
    received(PF, frecv.at[0:15])

    def whole_moments(means, squares):
        mean = jnp.sum(means, axis=0, keepdims=True) * (1.0 / N)
        apart = means - mean
        variance = (
            jnp.sum(squares, axis=0, keepdims=True)
            + 256.0 * jnp.sum(apart * apart, axis=0, keepdims=True)
        ) * (1.0 / 4096)
        return mean, apart, lax.rsqrt(variance + 1e-5)

    means = frecv[:, 0, :]
    mean, apart, scale = whole_moments(means, frecv[:, 1, :])
    mix = scale * jnp.sum(frecv[:, 2, :] + apart * frecv[:, 3, :], axis=0, keepdims=True)
    mix = 1.0 / (1.0 + jnp.exp(-mix))
    msend[...] = jnp.broadcast_to(mix, (2, 128))
    mrecv[e] = msend[...]
    hidden = (residual - to_column_of(mean)) * to_column_of(scale) * gain
    gsend[...] = hidden.astype(BF16)
    grecv[e] = gsend[...]
    over_ep(PG, lambda a: gsend, grecv.at[e])
    over_ep(PMIX, lambda a: msend, mrecv.at[e])

    arrived("eg", wgu.at[:, 0:2048])
    arrived("eu", wgu.at[:, 2048:4096])
    arrived("dg", wd.at[:, 0:128])
    arrived("du", wd.at[:, 128:256])
    received(PG, grecv.at[0:15])
    rows = grecv[...].reshape(256, 256)
    routed = dot(pick[...], rows).astype(BF16)
    hsend[:, 64:80, :] = dot(rows, wd[...]).astype(BF16).reshape(N, N, 256)

    def partial(b):
        hsend[b, 0:64, :] = dot(routed, wgu[:, chunk(b, 256)]).astype(BF16)

    def project(k, _):
        b = lax.rem(t + k, N)
        partial(b)
        send(PH, hsend.at[b], hrecv.at[t], (e, b))
        return 0

    lax.fori_loop(1, N, project, 0)
    partial(t)
    hrecv[t] = hsend[t]
    received(PH, hrecv.at[0:15])
    pre = jnp.sum(hrecv[...].astype(F32), axis=0)
    pre_gate = pre[:, 0:128]
    active = (pre_gate / (1.0 + jnp.exp(-pre_gate)) * pre[:, 128:256]).astype(BF16)
    isend[...] = active[0:64, :]
    isend2[...] = active[64:80, :]
    ihid[:, chunk(t, 128)] = isend[...]
    idense[t] = isend2[...]
    over_tp(PI, lambda b: isend, ihid.at[:, chunk(t, 128)])
    over_tp(PI2, lambda b: isend2, idense.at[t])

    received(PMIX, mrecv.at[0:15])
    mixes = mrecv[:, 0:1, :]
    own = lax.broadcasted_iota(jnp.int32, (N, N, 128), 1) == lax.broadcasted_iota(
        jnp.int32, (N, N, 128), 2
    )
    mix_col = jnp.sum(
        jnp.where(own, jnp.broadcast_to(mixes, (N, N, 128)), 0.0), axis=2, keepdims=True
    ).reshape(256, 1)

    arrived("ed", ed)
    arrived("dd", dd)
    received(PI2, idense.at[0:15])
    dense = dot(idense[...].reshape(256, 128), dd[...]) * mix_col
    received(PI, ihid.at[:, 0 : 15 * 128])
    result = dot(ihid[...], ed[...]).astype(BF16)
    mixture = dot(place[...], result) * gates[...] + dense
    jsend[...] = mixture.astype(BF16).reshape(N, N, 256)
    jrecv[e] = jsend[e]
    over_ep(PJ, lambda a: jsend.at[a], jrecv.at[e])
    arrived("sgain", sgain)
    received(PJ, jrecv.at[0:15])
    combined = root * gsend[...].astype(F32) + jnp.sum(jrecv[...].astype(F32), axis=0)

    mean_b, _, square_b = block_moments(combined)
    ksend[0:1, :] = to_row(mean_b, N, 128)
    ksend[1:2, :] = to_row(square_b, N, 128)
    krecv[t] = ksend[...]
    over_tp(PK, lambda b: ksend, krecv.at[t])
    received(PK, krecv.at[0:15])
    mean, _, scale = whole_moments(krecv[:, 0, :], krecv[:, 1, :])
    last_gain = jnp.concatenate([sgain[0:1, :], sgain[1:2, :]], axis=1)
    out_ref[...] = (
        (combined - to_column_of(mean)) * to_column_of(scale) * last_gain
    ).astype(BF16)

    sent(PA, xcol.at[0:15])
    sent(PMETA, metas.at[0:15])
    sent(PB, bsend.at[0:15])
    sent(PD, drecv.at[0:15])
    sent(PE, esend.at[0:15])

    @pl.when(e != t)
    def _():
        sent(PE, esend.at[0])

    sent(PF, frecv.at[0:15])
    sent(PG, grecv.at[0:15])
    sent(PMIX, mrecv.at[0:15])
    sent(PH, hsend.at[0:15])
    sent(PI, ihid.at[:, 0 : 15 * 128])
    sent(PI2, idense.at[0:15])
    sent(PJ, jsend.at[0:15])
    sent(PK, krecv.at[0:15])


def to_column_of(row):
    same = lax.broadcasted_iota(jnp.int32, (N, 128), 0) == lax.broadcasted_iota(
        jnp.int32, (N, 128), 1
    )
    return jnp.sum(jnp.where(same, jnp.broadcast_to(row, (N, 128)), 0), axis=1, keepdims=True)


def on_device(
    tokens, query_weight, key_weight, value_weight, out_weight, head_lambda, head_gain,
    key_cache, value_cache, lengths, first_gain, second_gain, expert_ids, route_weights,
    expert_gate, expert_up, expert_down, dense_gate, dense_up, dense_down, dense_mix,
):
    anywhere = pl.BlockSpec(memory_space=pltpu.HBM)
    vmem = pltpu.VMEM
    scratch = [
        vmem((N, 4096), BF16),
        vmem((256, 512), BF16),
        vmem((256, 256), BF16),
        vmem((1, 2), F32),
        vmem((1, 128), F32),
        vmem((N, CACHE, 128), BF16),
        vmem((N, CACHE, 128), BF16),
        vmem((1, N), jnp.int32),
        vmem((32, 128), F32),
        vmem((2, 128), F32),
        vmem((2, N), jnp.int32),
        vmem((2, N), F32),
        vmem((256, 4096), BF16),
        vmem((2048, 256), BF16),
        vmem((256, 256), BF16),
        vmem((128, 256), BF16),
        vmem((32, 128), BF16),
        vmem((N, N, 256), BF16),
        vmem((N, 128), F32),
        vmem((N, N, 128), F32),
        vmem((N, N, 512), BF16),
        vmem((N, N, 512), BF16),
        vmem((128, 128), F32),
        vmem((N, 128), F32),
        vmem((N, 128), F32),
        vmem((N, 128), F32),
        vmem((N, 128), F32),
        vmem((N, 128), jnp.int32),
        vmem((N, 256), BF16),
        vmem((N, N, 256), BF16),
        vmem((N, N, 256), BF16),
        vmem((N, N, 256), BF16),
        vmem((4, 128), F32),
        vmem((N, 4, 128), F32),
        vmem((N, 256), BF16),
        vmem((N, N, 256), BF16),
        vmem((2, 128), F32),
        vmem((N, 2, 128), F32),
        vmem((32, 128), F32),
        vmem((N, 80, 256), BF16),
        vmem((N, 80, 256), BF16),
        vmem((64, 128), BF16),
        vmem((N, 128), BF16),
        vmem((64, 2048), BF16),
        vmem((N, N, 128), BF16),
        vmem((N, N, 256), BF16),
        vmem((N, N, 256), BF16),
        vmem((2, 128), F32),
        vmem((N, 2, 128), F32),
        vmem((64, 256), BF16),
        vmem((256, 64), BF16),
        vmem((256, 1), F32),
        pltpu.SemaphoreType.DMA((len(LOCALS),)),
        pltpu.SemaphoreType.DMA((PHASES,)),
        pltpu.SemaphoreType.DMA((PHASES,)),
        pltpu.SemaphoreType.REGULAR,
    ]
    return pl.pallas_call(
        kernel,
        out_shape=jax.ShapeDtypeStruct((N, 256), BF16),
        in_specs=[anywhere] * 21,
        out_specs=pl.BlockSpec(memory_space=pltpu.VMEM),
        scratch_shapes=scratch,
        compiler_params=pltpu.CompilerParams(
            collective_id=0, has_side_effects=True, vmem_limit_bytes=67_043_328
        ),
        name="layer",
    )(
        tokens,
        query_weight,
        key_weight,
        value_weight,
        out_weight,
        head_lambda.reshape(1, 2),
        head_gain.reshape(1, 128),
        key_cache.reshape(N, CACHE, 128),
        value_cache.reshape(N, CACHE, 128),
        lengths.reshape(1, N),
        first_gain.reshape(32, 128),
        second_gain.reshape(2, 128),
        expert_ids.T,
        route_weights.T,
        expert_gate.reshape(256, 2048),
        expert_up.reshape(256, 2048),
        expert_down.reshape(2048, 256),
        dense_gate,
        dense_up,
        dense_down,
        dense_mix.reshape(32, 128),
    )


def solution(mesh):
    return jax.shard_map(
        on_device,
        mesh=mesh,
        in_specs=(
            P("ep", None),
            P("ep", "tp"),
            P("ep", "tp"),
            P("ep", "tp"),
            P("tp", "ep"),
            P("tp"),
            P(),
            P("ep", None, "tp", None),
            P("ep", None, "tp", None),
            P("ep"),
            P(),
            P("tp"),
            P("ep", None),
            P("ep", None),
            P("ep", "tp", None),
            P("ep", "tp", None),
            P("ep", None, "tp"),
            P("tp", "ep"),
            P("tp", "ep"),
            P("ep", "tp"),
            P(),
        ),
        out_specs=P("ep", "tp"),
        check_vma=False,
    )
```

```python
import functools
import math

import jax
import jax.numpy as jnp
from jax import lax
from jax.experimental import pallas as pl
from jax.experimental.pallas import tpu as pltpu
from jax.sharding import PartitionSpec as P

N = 16
CACHE = 1024
CAP = 4
F32 = jnp.float32
BF16 = jnp.bfloat16
MESH = pl.DeviceIdType.MESH

(
    PA, PMETA, PB, PW1, PW2, PWGU, PWD, PE, PMEAN, PF, PG, PS, PX, PXR, PH, PI, PID, PC, PCD, PJ, PK,
) = range(21)
PHASES = 21

LOCALS = (
    "tok", "qw", "kw", "vw", "ow", "lam", "hgain", "kc", "vc", "lens", "fgain",
    "sgain", "ids", "rw", "eg", "eu", "ed", "dg", "du", "dd", "dmix",
)


def dot(a, b):
    return jnp.dot(a, b, preferred_element_type=F32)


def to_column(row, n):
    same = lax.broadcasted_iota(jnp.int32, (n, n), 0) == lax.broadcasted_iota(jnp.int32, (n, n), 1)
    return jnp.sum(jnp.where(same, jnp.broadcast_to(row, (n, n)), 0), axis=1, keepdims=True)


def to_row(column, n, lanes):
    same = lax.broadcasted_iota(jnp.int32, (n, lanes), 0) == lax.broadcasted_iota(
        jnp.int32, (n, lanes), 1
    )
    return jnp.sum(jnp.where(same, jnp.broadcast_to(column, (n, lanes)), 0), axis=0, keepdims=True)


def slot_of(i):
    return lax.rem(i, 2) * 8 + i // 2


def kernel(
    tok_h, qw_h, kw_h, vw_h, ow_h, lam_h, hgain_h, kc_h, vc_h, lens_h, fgain_h, sgain_h,
    ids_h, rw_h, eg_h, eu_h, ed_h, dg_h, du_h, dd_h, dmix_h,
    out_ref,
    tok, wqkv, wo, lam, hgain, kc, vc, lens, fgain, sgain, ids, rw, wgu, wgu2, ed, wd, wd2, dd, dmix,
    xcol, meta, metas, bsend, brecv, qs, kn, vn, h0, h1, lens_b, normed, esend, erecv,
    asend, arecv, fsend, frecv, gsend, grecv, ssend, srecv, gw, xsend, xrecv, xrows,
    hsend, hrecv, isend, idsend, ihid, idense,
    jsend, jrecv, ksend, krecv, pick, place, gates,
    lsem, ssem, rsem,
):
    e = lax.axis_index("ep")
    t = lax.axis_index("tp")
    z, c = t // 2, lax.rem(t, 2)
    partner = (e, 2 * z + 1 - c)
    y, x = e // 4, lax.rem(e, 4)
    e_slot = slot_of(e)

    def chunk(i, width):
        return pl.ds(pl.multiple_of(i * width, width), width)

    coming, flights = {}, []

    def bring(name, pairs, whole=None):
        sem = lsem.at[LOCALS.index(name)]
        coming[name] = pairs[0][1] if whole is None else whole
        for src, dst in pairs:
            pltpu.make_async_copy(src, dst, sem).start()

    def arrived(name):
        whole = coming.pop(name)
        pltpu.make_async_copy(whole, whole, lsem.at[LOCALS.index(name)]).wait()

    bring("tok", [(tok_h, tok)])
    bring("ids", [(ids_h, ids)])
    bring("rw", [(rw_h, rw)])
    bring("ow", [(ow_h, wo.at[y, x])])
    bring("qw", [(qw_h, wqkv.at[:, 0:256])])
    bring("kw", [(kw_h, wqkv.at[:, 256:384])])
    bring("vw", [(vw_h, wqkv.at[:, 384:512])])
    bring("lens", [(lens_h, lens)])
    bring("lam", [(lam_h, lam)])
    bring("hgain", [(hgain_h, hgain)])
    bring("fgain", [(fgain_h, fgain)])
    bring("dmix", [(dmix_h, dmix)])
    bring("sgain", [(sgain_h, sgain)])

    def bring_pair(i, _):
        sem_g = lsem.at[LOCALS.index("eg")]
        sem_u = lsem.at[LOCALS.index("eu")]
        core, chip = lax.rem(i, 2), i // 2
        even = pl.ds(pl.multiple_of(chip * 256, 256), 128)
        odd = pl.ds(pl.multiple_of(chip * 256 + 128, 128), 128)
        pltpu.make_async_copy(eg_h.at[:, chunk(i, 128)], wgu.at[core, :, even], sem_g).start()
        pltpu.make_async_copy(eu_h.at[:, chunk(i, 128)], wgu.at[core, :, odd], sem_u).start()
        return 0

    lax.fori_loop(0, N, bring_pair, 0)
    coming["eg"] = wgu.at[0]
    coming["eu"] = wgu.at[1]
    bring("dg", [(dg_h, wd.at[:, 0:128])])
    bring("du", [(du_h, wd.at[:, 128:256])])
    bring("kc", [(kc_h, kc)])
    bring("vc", [(vc_h, vc)])

    def bring_down(i, _):
        core, chip = lax.rem(i, 2), i // 2
        pltpu.make_async_copy(
            ed_h.at[chunk(i, 128), :], ed.at[core, chunk(chip, 128), :], lsem.at[LOCALS.index("ed")]
        ).start()
        return 0

    lax.fori_loop(0, N, bring_down, 0)
    coming["ed"] = ed
    bring("dd", [(dd_h, dd)])

    barrier = pltpu.get_barrier_semaphore()

    def greet(k, _):
        pl.semaphore_signal(
            barrier, inc=1, device_id=(lax.rem(e + k, N), t), device_id_type=MESH
        )
        pl.semaphore_signal(
            barrier, inc=1, device_id=(e, lax.rem(t + k, N)), device_id_type=MESH
        )
        return 0

    lax.fori_loop(1, N, greet, 0)

    def send(phase, src, dst, to):
        pltpu.make_async_remote_copy(
            src_ref=src,
            dst_ref=dst,
            send_sem=ssem.at[phase],
            recv_sem=rsem.at[phase],
            device_id=to,
            device_id_type=MESH,
        ).start()

    def over_ep(phase, src_of, dst):
        def one(k, _):
            a = lax.rem(e + k, N)
            send(phase, src_of(a), dst, (a, t))
            return 0

        lax.fori_loop(1, N, one, 0)

    def far_first(i, n):
        half = (i + 1) // 2
        return n // 2 + half * (2 * lax.rem(i + 1, 2) - 1)

    def over_tp(phase, src_of, dst):
        def one(i, _):
            b = lax.rem(t + far_first(i, N), N)
            send(phase, src_of(b), dst, (e, b))
            return 0

        lax.fori_loop(0, N - 1, one, 0)

    def over_z(phase, src_of, dst):
        def one(i, _):
            chip = lax.rem(z + far_first(i, 8), 8)
            send(phase, src_of(chip), dst, (e, 2 * chip + c))
            return 0

        lax.fori_loop(0, 7, one, 0)

    def received(phase, blocks):
        pltpu.make_async_copy(blocks, blocks, rsem.at[phase]).wait()

    def sent(phase, blocks):
        pltpu.make_async_copy(blocks, blocks, ssem.at[phase]).wait()

    lane = lax.broadcasted_iota(jnp.int32, (N, 128), 1)

    arrived("ids")
    arrived("rw")
    id0 = to_column(ids[0:1, :], N)
    id1 = to_column(ids[1:2, :], N)
    w0 = to_column(rw[0:1, :], N)
    w1 = to_column(rw[1:2, :], N)
    total = w0 + w1
    hit0 = lane == id0
    hit1 = lane == id1
    hit = jnp.where(hit0 | hit1, 1.0, 0.0).astype(F32)
    before = jnp.where(
        lax.broadcasted_iota(jnp.int32, (N, N), 1) < lax.broadcasted_iota(jnp.int32, (N, N), 0),
        1.0,
        0.0,
    ).astype(F32)
    slot = dot(before.astype(BF16), hit.astype(BF16))
    code = jnp.where(hit > 0.5, slot, -1.0)
    gate0 = jnp.where(lane - N == id0, w0 / total, 0.0)
    gate1 = jnp.where(lane - N == id1, w1 / total, 0.0)
    meta[...] = jnp.where(lane < N, code, gate0 + gate1)
    metas[e_slot] = meta[...]

    arrived("lens")
    length = to_column(lens[...], N)
    lens_b[...] = jnp.broadcast_to(length, (N, 128))
    turn = lax.rem(lane, 32).astype(F32) * (2.0 / 64)
    angle = length.astype(F32) * jnp.exp(turn * (-math.log(500000.0)))
    low = lax.rem(lane, 64) < 32
    cosine = jnp.cos(angle)
    sine = jnp.sin(angle)
    sine = jnp.where(low, -sine, sine)

    arrived("tok")
    xcol[e] = tok[:, chunk(e, 256)]
    arrived("ow")

    pl.semaphore_wait(barrier, 2 * (N - 1))

    over_ep(PA, lambda a: tok.at[:, chunk(a, 256)], xcol.at[e])
    flights.append((PA, xcol.at[0:15]))

    def first_half(k, _):
        send(PW1, wo.at[y, x, 0:128], wo.at[y, x, 0:128], (4 * y + lax.rem(x + k, 4), t))
        send(PW1, wo.at[y, x, 128:256], wo.at[y, x, 128:256], (4 * lax.rem(y + k, 4) + x, t))
        return 0

    lax.fori_loop(1, 4, first_half, 0)
    flights.append((PW1, wo.at[0, 0:3]))

    arrived("qw")
    arrived("kw")
    arrived("vw")
    received(PA, xcol.at[0:15])
    bsend[...] = dot(xcol[...].reshape(256, 256), wqkv[...]).astype(BF16).reshape(N, N, 512)
    brecv[e] = bsend[e]
    over_ep(PB, lambda a: bsend.at[a], brecv.at[e])
    flights.append((PB, bsend.at[0:15]))
    over_ep(PMETA, lambda a: meta, metas.at[e_slot])
    flights.append((PMETA, metas.at[0:15]))

    received(PW1, wo.at[0, 0:3])

    def second_half(k, _):
        send(PW2, wo.at[y, :, 0:128], wo.at[y, :, 0:128], (4 * lax.rem(y + k, 4) + x, t))
        send(PW2, wo.at[:, x, 128:256], wo.at[:, x, 128:256], (4 * y + lax.rem(x + k, 4), t))
        return 0

    lax.fori_loop(1, 4, second_half, 0)
    flights.append((PW2, wo.at[0:3]))

    arrived("eg")
    arrived("eu")
    arrived("dg")
    arrived("du")
    send(PWGU, wgu.at[1 - c], wgu2, partner)
    flights.append((PWGU, wgu2))
    send(PWD, wd, wd2, partner)
    flights.append((PWD, wd2))

    received(PB, brecv.at[0:15])
    qkv = jnp.sum(brecv[...].astype(F32), axis=0).astype(BF16).astype(F32)

    def rotated(v):
        swapped = jnp.where(low, pltpu.roll(v, 96, 1), pltpu.roll(v, 32, 1))
        return (v * cosine + swapped * sine).astype(BF16).astype(F32)

    first = lane < 64
    qs[...] = jnp.zeros_like(qs)
    for g in range(2):
        q = rotated(qkv[:, g * 128 : (g + 1) * 128]) * 0.125
        qs[pl.ds(g, N, stride=8), :] = jnp.where(first, q, 0.0)
        qs[pl.ds(g + 4, N, stride=8), :] = jnp.where(first, 0.0, q)
    kn[...] = rotated(qkv[:, 256:384])
    vn[...] = qkv[:, 384:512]

    arrived("lam")
    row8 = lax.broadcasted_iota(jnp.int32, (8, 1), 0)
    share = jnp.where(row8 == 4, -lam[0:1, 0:1], jnp.where(row8 == 5, -lam[0:1, 1:2], 1.0))
    place_of = lax.broadcasted_iota(jnp.int32, (8, CACHE), 1)

    arrived("kc")
    arrived("vc")

    def attend(s):
        q = qs[pl.ds(pl.multiple_of(s * 8, 8), 8), :]
        scores = lax.dot_general(
            q.astype(BF16), kc[s], (((1,), (1,)), ((), ())), preferred_element_type=F32
        )
        fresh = jnp.sum(q * kn[pl.ds(s, 1), :], axis=1, keepdims=True)
        scores = jnp.where(place_of < lens_b[pl.ds(s, 1), 0:1], scores, -1e30)
        top = jnp.maximum(jnp.max(scores, axis=1, keepdims=True), fresh)
        p = jnp.exp(scores - top)
        fresh_p = jnp.exp(fresh - top)
        scale = share / (jnp.sum(p, axis=1, keepdims=True) + fresh_p)
        p = p * scale
        fresh_p = fresh_p * scale
        p = p + pltpu.roll(p, 4, 0)
        fresh_p = jnp.broadcast_to(fresh_p, (8, 128))
        fresh_p = (fresh_p + pltpu.roll(fresh_p, 4, 0)).astype(BF16).astype(F32)
        head = dot(p.astype(BF16), vc[s]) + fresh_p * vn[pl.ds(s, 1), :]
        h0[pl.ds(s, 1), :] = head[0:1, :]
        h1[pl.ds(s, 1), :] = head[1:2, :]

    def attend_some(i, _):
        for j in range(4):
            attend(i * 4 + j)
        return 0

    lax.fori_loop(0, N // 4, attend_some, 0)

    arrived("hgain")
    for g, ref in enumerate((h0, h1)):
        head = ref[...]
        mean = jnp.mean(head * head, axis=1, keepdims=True)
        head = head * lax.rsqrt(mean + 1e-6) * hgain[...] * 0.8
        normed[:, g * 128 : (g + 1) * 128] = head.astype(BF16)
    received(PW2, wo.at[0:3])

    def out_block(b):
        part = dot(normed[...], wo[b // 4, lax.rem(b, 4)])
        esend[b] = part.astype(BF16)
        return part

    def out_send(i, sums):
        b = lax.rem(t + far_first(i, N), N)
        part = out_block(b)
        send(PE, esend.at[b], erecv.at[t], (e, b))
        return sums + part

    sums = lax.fori_loop(0, N - 1, out_send, jnp.zeros((N, 256), F32))
    flights.append((PE, esend.at[0:15]))
    sums = jnp.sum(sums + out_block(t), axis=1, keepdims=True)
    erecv[t] = esend[t]
    asend[...] = to_row(sums, N, 128)
    arecv[t] = asend[...]
    over_tp(PMEAN, lambda b: asend, arecv.at[t])
    flights.append((PMEAN, arecv.at[0:15]))

    received(PMETA, metas.at[0:15])
    every = metas[...].reshape(256, 128)
    wide_lane = lax.broadcasted_iota(jnp.int32, (256, 128), 1)
    code_col = jnp.sum(jnp.where(wide_lane == e, every, 0.0), axis=1, keepdims=True)
    gate_col = jnp.sum(jnp.where(wide_lane == e + N, every, 0.0), axis=1, keepdims=True)
    block = (lax.broadcasted_iota(jnp.int32, (256, 1), 0) // N * CAP).astype(F32)
    target = jnp.where(code_col >= 0.0, code_col + block, -1.0)
    place[...] = jnp.where(
        lax.broadcasted_iota(jnp.int32, (256, 64), 1).astype(F32) == target, 1.0, 0.0
    ).astype(BF16)
    pick[...] = jnp.where(
        lax.broadcasted_iota(jnp.int32, (64, 256), 0).astype(F32) == to_row(target, 256, 256),
        1.0,
        0.0,
    ).astype(BF16)
    gates[...] = gate_col

    arrived("fgain")
    arrived("dmix")
    gw[...] = fgain[...] * dmix[...].astype(F32)

    def block_of(ref):
        return jnp.concatenate([ref[pl.ds(2 * t, 1), :], ref[pl.ds(2 * t + 1, 1), :]], axis=1)

    gain = block_of(fgain)
    gain_mix = block_of(gw)
    root = 2.0**0.5
    token_mean = root * jnp.mean(tok[...].astype(F32), axis=1, keepdims=True)
    own_tokens = root * tok[:, chunk(t, 256)].astype(F32)

    received(PE, erecv.at[0:15])
    residual = own_tokens + jnp.sum(erecv[...].astype(F32), axis=0)
    received(PMEAN, arecv.at[0:15])
    mean = token_mean + to_column_of(jnp.sum(arecv[...], axis=0)) * (1.0 / 4096)
    centred = residual - mean
    gsend[...] = (centred * gain).astype(BF16)
    grecv[e_slot] = gsend[...]
    over_ep(PG, lambda a: gsend, grecv.at[e_slot])
    flights.append((PG, grecv.at[0:15]))
    fsend[0:1, :] = to_row(jnp.sum(centred * centred, axis=1, keepdims=True), N, 128)
    fsend[1:2, :] = to_row(jnp.sum(centred * gain_mix, axis=1, keepdims=True), N, 128)
    frecv[t] = fsend[...]
    over_tp(PF, lambda b: fsend, frecv.at[t])
    flights.append((PF, frecv.at[0:15]))

    received(PG, grecv.at[0:15])
    xsend[...] = dot(pick[...], grecv[...].reshape(256, 256)).astype(BF16)
    send(PX, xsend, xrecv, partner)
    flights.append((PX, xrecv))
    send(PXR, grecv.at[pl.ds((1 - c) * 8, 8)], xrows, partner)
    flights.append((PXR, xrows))

    received(PF, frecv.at[0:15])
    totals = jnp.sum(frecv[...], axis=0)
    scale_row = lax.rsqrt(totals[0:1, :] * (1.0 / 4096) + 1e-5)
    mix = 1.0 / (1.0 + jnp.exp(-scale_row * totals[1:2, :]))
    ssend[0:1, :] = scale_row
    ssend[1:2, :] = mix
    srecv[e_slot] = ssend[...]
    over_ep(PS, lambda a: ssend, srecv.at[e_slot])
    flights.append((PS, srecv.at[0:15]))

    received(PWGU, wgu2)
    received(PWD, wd2)
    received(PX, xrecv)
    received(PXR, xrows)
    mine = grecv[pl.ds(c * 8, 8)].reshape(128, 256)
    dense_pre = dot(mine, wd[...]) + dot(xrows[...].reshape(128, 256), wd2[...])
    hsend[:, 64:80, :] = dense_pre.astype(BF16).reshape(8, N, 256)

    def partial(chip):
        cols = chunk(chip, 256)
        pre = dot(xsend[...], wgu[c, :, cols]) + dot(xrecv[...], wgu2[:, cols])
        hsend[chip, 0:64, :] = pre.astype(BF16)

    def project(i, _):
        chip = lax.rem(z + far_first(i, 8), 8)
        partial(chip)
        send(PH, hsend.at[chip], hrecv.at[z], (e, 2 * chip + c))
        return 0

    lax.fori_loop(0, 7, project, 0)
    flights.append((PH, hsend.at[0:7]))
    partial(z)
    hrecv[z] = hsend[z]

    received(PS, srecv.at[0:15])
    own = lax.broadcasted_iota(jnp.int32, (N, N, 128), 1) == lax.broadcasted_iota(
        jnp.int32, (N, N, 128), 2
    )

    def token_column(rows):
        spread = jnp.where(own, jnp.broadcast_to(rows, (N, N, 128)), 0.0)
        return jnp.sum(spread, axis=2, keepdims=True).reshape(256, 1)

    mix_col = token_column(srecv[:, 1:2, :])
    scale_col = token_column(srecv[:, 0:1, :])
    row_scale = to_column(
        jnp.sum(jnp.where(place[...].astype(F32) > 0.5, scale_col, 0.0), axis=0, keepdims=True), 64
    )
    dense_scale = to_column_of(srecv[slot_of(t), 0:1, :])
    all_scale = jnp.concatenate([row_scale, dense_scale], axis=0)
    hidden = centred * to_column_of(scale_row) * gain

    received(PH, hrecv.at[0:7])
    pre = jnp.sum(hrecv[...].astype(F32), axis=0) * all_scale
    pre_gate = pre[:, 0:128]
    active = (pre_gate / (1.0 + jnp.exp(-pre_gate)) * pre[:, 128:256]).astype(BF16)
    isend[...] = active[0:64, :]
    idsend[...] = active[64:80, :]
    ihid[c, :, chunk(z, 128)] = isend[...]
    idense[c * 8 + z] = idsend[...]
    over_z(PI, lambda chip: isend, ihid.at[c, :, chunk(z, 128)])
    flights.append((PI, ihid.at[0, :, 0 : 7 * 128]))
    over_z(PID, lambda chip: idsend, idense.at[c * 8 + z])
    flights.append((PID, idense.at[0:7]))
    arrived("ed")
    arrived("dd")
    received(PI, ihid.at[0, :, 0 : 7 * 128])
    send(PC, ihid.at[c], ihid.at[c], partner)
    flights.append((PC, ihid.at[0]))
    received(PID, idense.at[0:7])
    send(PCD, idense.at[pl.ds(c * 8, 8)], idense.at[pl.ds(c * 8, 8)], partner)
    flights.append((PCD, idense.at[0:8]))
    result = dot(ihid[c], ed[c])
    received(PC, ihid.at[0])
    received(PCD, idense.at[0:8])
    result = (result + dot(ihid[1 - c], ed[1 - c])).astype(BF16)
    dense = dot(idense[...].reshape(256, 128), dd[...]) * mix_col
    mixture = dot(place[...], result) * gates[...] + dense
    jsend[...] = mixture.astype(BF16).reshape(N, N, 256)
    jrecv[e] = jsend[e_slot]
    over_ep(PJ, lambda a: jsend.at[slot_of(a)], jrecv.at[e])
    flights.append((PJ, jsend.at[0:15]))
    arrived("sgain")
    received(PJ, jrecv.at[0:15])
    combined = root * hidden.astype(BF16).astype(F32) + jnp.sum(jrecv[...].astype(F32), axis=0)

    mean_b = jnp.sum(combined, axis=1, keepdims=True) * (1.0 / 256)
    apart = combined - mean_b
    ksend[0:1, :] = to_row(mean_b, N, 128)
    ksend[1:2, :] = to_row(jnp.sum(apart * apart, axis=1, keepdims=True), N, 128)
    krecv[t] = ksend[...]
    over_tp(PK, lambda b: ksend, krecv.at[t])
    flights.append((PK, krecv.at[0:15]))
    received(PK, krecv.at[0:15])
    means = krecv[:, 0, :]
    mean = jnp.sum(means, axis=0, keepdims=True) * (1.0 / N)
    off = means - mean
    square = jnp.sum(krecv[:, 1, :] + 256.0 * off * off, axis=0, keepdims=True)
    scale = lax.rsqrt(square * (1.0 / 4096) + 1e-5)
    last_gain = jnp.concatenate([sgain[0:1, :], sgain[1:2, :]], axis=1)
    out_ref[...] = (
        (combined - to_column_of(mean)) * to_column_of(scale) * last_gain
    ).astype(BF16)

    for phase, blocks in flights:
        sent(phase, blocks)


def to_column_of(row):
    same = lax.broadcasted_iota(jnp.int32, (N, 128), 0) == lax.broadcasted_iota(
        jnp.int32, (N, 128), 1
    )
    return jnp.sum(jnp.where(same, jnp.broadcast_to(row, (N, 128)), 0), axis=1, keepdims=True)


def on_device(
    tokens, query_weight, key_weight, value_weight, out_weight, head_lambda, head_gain,
    key_cache, value_cache, lengths, first_gain, second_gain, expert_ids, route_weights,
    expert_gate, expert_up, expert_down, dense_gate, dense_up, dense_down, dense_mix,
):
    anywhere = pl.BlockSpec(memory_space=pltpu.HBM)
    vmem = pltpu.VMEM
    scratch = [
        vmem((N, 4096), BF16),
        vmem((256, 512), BF16),
        vmem((4, 4, 256, 256), BF16),
        vmem((1, 2), F32),
        vmem((1, 128), F32),
        vmem((N, CACHE, 128), BF16),
        vmem((N, CACHE, 128), BF16),
        vmem((1, N), jnp.int32),
        vmem((32, 128), F32),
        vmem((2, 128), F32),
        vmem((2, N), jnp.int32),
        vmem((2, N), F32),
        vmem((2, 256, 2048), BF16),
        vmem((256, 2048), BF16),
        vmem((2, 1024, 256), BF16),
        vmem((256, 256), BF16),
        vmem((256, 256), BF16),
        vmem((128, 256), BF16),
        vmem((32, 128), BF16),
        vmem((N, N, 256), BF16),
        vmem((N, 128), F32),
        vmem((N, N, 128), F32),
        vmem((N, N, 512), BF16),
        vmem((N, N, 512), BF16),
        vmem((128, 128), F32),
        vmem((N, 128), F32),
        vmem((N, 128), F32),
        vmem((N, 128), F32),
        vmem((N, 128), F32),
        vmem((N, 128), jnp.int32),
        vmem((N, 256), BF16),
        vmem((N, N, 256), BF16),
        vmem((N, N, 256), BF16),
        vmem((1, 128), F32),
        vmem((N, 1, 128), F32),
        vmem((2, 128), F32),
        vmem((N, 2, 128), F32),
        vmem((N, 256), BF16),
        vmem((N, N, 256), BF16),
        vmem((2, 128), F32),
        vmem((N, 2, 128), F32),
        vmem((32, 128), F32),
        vmem((64, 256), BF16),
        vmem((64, 256), BF16),
        vmem((8, N, 256), BF16),
        vmem((8, 80, 256), BF16),
        vmem((8, 80, 256), BF16),
        vmem((64, 128), BF16),
        vmem((N, 128), BF16),
        vmem((2, 64, 1024), BF16),
        vmem((N, N, 128), BF16),
        vmem((N, N, 256), BF16),
        vmem((N, N, 256), BF16),
        vmem((2, 128), F32),
        vmem((N, 2, 128), F32),
        vmem((64, 256), BF16),
        vmem((256, 64), BF16),
        vmem((256, 1), F32),
        pltpu.SemaphoreType.DMA((len(LOCALS),)),
        pltpu.SemaphoreType.DMA((PHASES,)),
        pltpu.SemaphoreType.DMA((PHASES,)),
    ]
    return pl.pallas_call(
        kernel,
        out_shape=jax.ShapeDtypeStruct((N, 256), BF16),
        in_specs=[anywhere] * 21,
        out_specs=pl.BlockSpec(memory_space=pltpu.VMEM),
        scratch_shapes=scratch,
        compiler_params=pltpu.CompilerParams(
            collective_id=0, has_side_effects=True, vmem_limit_bytes=67_043_328
        ),
        name="layer",
    )(
        tokens,
        query_weight,
        key_weight,
        value_weight,
        out_weight,
        head_lambda.reshape(1, 2),
        head_gain.reshape(1, 128),
        key_cache.reshape(N, CACHE, 128),
        value_cache.reshape(N, CACHE, 128),
        lengths.reshape(1, N),
        first_gain.reshape(32, 128),
        second_gain.reshape(2, 128),
        expert_ids.T,
        route_weights.T,
        expert_gate.reshape(256, 2048),
        expert_up.reshape(256, 2048),
        expert_down.reshape(2048, 256),
        dense_gate,
        dense_up,
        dense_down,
        dense_mix.reshape(32, 128),
    )


def solution(mesh):
    return jax.shard_map(
        on_device,
        mesh=mesh,
        in_specs=(
            P("ep", None),
            P("ep", "tp"),
            P("ep", "tp"),
            P("ep", "tp"),
            P("tp", "ep"),
            P("tp"),
            P(),
            P("ep", None, "tp", None),
            P("ep", None, "tp", None),
            P("ep"),
            P(),
            P("tp"),
            P("ep", None),
            P("ep", None),
            P("ep", "tp", None),
            P("ep", "tp", None),
            P("ep", None, "tp"),
            P("tp", "ep"),
            P("tp", "ep"),
            P("ep", "tp"),
            P(),
        ),
        out_specs=P("ep", "tp"),
        check_vma=False,
    )
```

```python
import functools
import math

import jax
import jax.numpy as jnp
from jax import lax
from jax.experimental import pallas as pl
from jax.experimental.pallas import tpu as pltpu
from jax.sharding import PartitionSpec as P

N = 16
CACHE = 1024
CAP = 4
F32 = jnp.float32
BF16 = jnp.bfloat16
MESH = pl.DeviceIdType.MESH

(
    PA, PMETA, PB, PV, PW1, PW2, PWGU, PWD, PD, PE, PMEAN, PF, PG, PS, PX, PXR, PH, PI, PID, PC, PCD, PJ, PK,
) = range(23)
PHASES = 23

LOCALS = (
    "tok", "qw", "kw", "vw", "ow", "lam", "hgain", "kc", "vc", "lens", "fgain",
    "sgain", "ids", "rw", "eg", "eu", "ed", "dg", "du", "dd", "dmix",
)


def dot(a, b):
    return jnp.dot(a, b, preferred_element_type=F32)


def to_column(row, n):
    same = lax.broadcasted_iota(jnp.int32, (n, n), 0) == lax.broadcasted_iota(jnp.int32, (n, n), 1)
    return jnp.sum(jnp.where(same, jnp.broadcast_to(row, (n, n)), 0), axis=1, keepdims=True)


def to_row(column, n, lanes):
    same = lax.broadcasted_iota(jnp.int32, (n, lanes), 0) == lax.broadcasted_iota(
        jnp.int32, (n, lanes), 1
    )
    return jnp.sum(jnp.where(same, jnp.broadcast_to(column, (n, lanes)), 0), axis=0, keepdims=True)


def slot_of(i):
    return lax.rem(i, 2) * 8 + i // 2


def kernel(
    tok_h, qw_h, kw_h, vw_h, ow_h, lam_h, hgain_h, kc_h, vc_h, lens_h, fgain_h, sgain_h,
    ids_h, rw_h, eg_h, eu_h, ed_h, dg_h, du_h, dd_h, dmix_h,
    out_ref,
    tok, wqkv, wo, lam, hgain, kc, vc, lens, fgain, sgain, ids, rw, wgu, wgu2, ed, wd, wd2, dd, dmix,
    xcol, meta, metas, bsend, brecv, qd, scores, normed, dnorm, vsend, vrecv, esend, erecv,
    asend, arecv, fsend, frecv, gsend, grecv, ssend, srecv, gw, xsend, xrecv, xrows,
    hsend, hrecv, isend, idsend, ihid, idense,
    jsend, jrecv, ksend, krecv, pick, place, gates,
    lsem, ssem, rsem, ready,
):
    e = lax.axis_index("ep")
    t = lax.axis_index("tp")
    z, c = t // 2, lax.rem(t, 2)
    partner = (e, 2 * z + 1 - c)
    y, x = e // 4, lax.rem(e, 4)
    e_slot = slot_of(e)

    def chunk(i, width):
        return pl.ds(pl.multiple_of(i * width, width), width)

    barrier = pltpu.get_barrier_semaphore()

    def greet(k, _):
        pl.semaphore_signal(
            barrier, inc=1, device_id=(lax.rem(e + k, N), t), device_id_type=MESH
        )
        pl.semaphore_signal(
            barrier, inc=1, device_id=(e, lax.rem(t + k, N)), device_id_type=MESH
        )
        return 0

    lax.fori_loop(1, N, greet, 0)

    coming, flights = {}, []

    def bring(name, pairs, whole=None):
        sem = lsem.at[LOCALS.index(name)]
        coming[name] = pairs[0][1] if whole is None else whole
        for src, dst in pairs:
            pltpu.make_async_copy(src, dst, sem).start()

    def arrived(name):
        whole = coming.pop(name)
        pltpu.make_async_copy(whole, whole, lsem.at[LOCALS.index(name)]).wait()

    bring("tok", [(tok_h, tok)])
    bring("ids", [(ids_h, ids)])
    bring("rw", [(rw_h, rw)])
    bring("ow", [(ow_h, wo.at[x])])
    bring("qw", [(qw_h, wqkv.at[:, 0:256])])
    bring("kw", [(kw_h, wqkv.at[:, 256:384])])
    bring("vw", [(vw_h, wqkv.at[:, 384:512])])
    bring("lens", [(lens_h, lens)])
    bring("lam", [(lam_h, lam)])
    bring("hgain", [(hgain_h, hgain)])
    bring("fgain", [(fgain_h, fgain)])
    bring("dmix", [(dmix_h, dmix)])
    bring("sgain", [(sgain_h, sgain)])

    def bring_pair(i, _):
        sem_g = lsem.at[LOCALS.index("eg")]
        sem_u = lsem.at[LOCALS.index("eu")]
        core, chip = lax.rem(i, 2), i // 2
        even = pl.ds(pl.multiple_of(chip * 256, 256), 128)
        odd = pl.ds(pl.multiple_of(chip * 256 + 128, 128), 128)
        pltpu.make_async_copy(eg_h.at[:, chunk(i, 128)], wgu.at[core, :, even], sem_g).start()
        pltpu.make_async_copy(eu_h.at[:, chunk(i, 128)], wgu.at[core, :, odd], sem_u).start()
        return 0

    lax.fori_loop(0, N, bring_pair, 0)
    coming["eg"] = wgu.at[0]
    coming["eu"] = wgu.at[1]
    bring("dg", [(dg_h, wd.at[:, 0:128])])
    bring("du", [(du_h, wd.at[:, 128:256])])
    bring("kc", [(kc_h.at[s], kc.at[:, s * 128 : (s + 1) * 128]) for s in range(N)], kc)
    bring("vc", [(vc_h.at[s], vc.at[:, s * 128 : (s + 1) * 128]) for s in range(N)], vc)

    def bring_down(i, _):
        core, chip = lax.rem(i, 2), i // 2
        pltpu.make_async_copy(
            ed_h.at[chunk(i, 128), :], ed.at[core, chunk(chip, 128), :], lsem.at[LOCALS.index("ed")]
        ).start()
        return 0

    lax.fori_loop(0, N, bring_down, 0)
    coming["ed"] = ed
    bring("dd", [(dd_h, dd)])

    def send(phase, src, dst, to):
        pltpu.make_async_remote_copy(
            src_ref=src,
            dst_ref=dst,
            send_sem=ssem.at[phase],
            recv_sem=rsem.at[phase],
            device_id=to,
            device_id_type=MESH,
        ).start()

    def over_ep(phase, src_of, dst):
        def one(k, _):
            a = lax.rem(e + k, N)
            send(phase, src_of(a), dst, (a, t))
            return 0

        lax.fori_loop(1, N, one, 0)

    def far_first(i, n):
        half = (i + 1) // 2
        return n // 2 + half * (2 * lax.rem(i + 1, 2) - 1)

    def over_tp(phase, src_of, dst):
        def one(i, _):
            b = lax.rem(t + far_first(i, N), N)
            send(phase, src_of(b), dst, (e, b))
            return 0

        lax.fori_loop(0, N - 1, one, 0)

    def over_z(phase, src_of, dst):
        def one(i, _):
            chip = lax.rem(z + far_first(i, 8), 8)
            send(phase, src_of(chip), dst, (e, 2 * chip + c))
            return 0

        lax.fori_loop(0, 7, one, 0)

    def received(phase, blocks):
        pltpu.make_async_copy(blocks, blocks, rsem.at[phase]).wait()

    def sent(phase, blocks):
        pltpu.make_async_copy(blocks, blocks, ssem.at[phase]).wait()

    lane = lax.broadcasted_iota(jnp.int32, (N, 128), 1)

    arrived("ids")
    arrived("rw")
    id0 = to_column(ids[0:1, :], N)
    id1 = to_column(ids[1:2, :], N)
    w0 = to_column(rw[0:1, :], N)
    w1 = to_column(rw[1:2, :], N)
    total = w0 + w1
    hit0 = lane == id0
    hit1 = lane == id1
    hit = jnp.where(hit0 | hit1, 1.0, 0.0).astype(F32)
    before = jnp.where(
        lax.broadcasted_iota(jnp.int32, (N, N), 1) < lax.broadcasted_iota(jnp.int32, (N, N), 0),
        1.0,
        0.0,
    ).astype(F32)
    slot = dot(before.astype(BF16), hit.astype(BF16))
    code = jnp.where(hit > 0.5, slot, -1.0)
    gate0 = jnp.where(lane - N == id0, w0 / total, 0.0)
    gate1 = jnp.where(lane - N == id1, w1 / total, 0.0)
    meta[...] = jnp.where(lane < N, code, gate0 + gate1)
    metas[e_slot] = meta[...]

    arrived("lens")
    length = to_column(lens[...], N)
    turn = lax.rem(lane, 32).astype(F32) * (2.0 / 64)
    angle = length.astype(F32) * jnp.exp(turn * (-math.log(500000.0)))
    low = lax.rem(lane, 64) < 32
    cosine = jnp.cos(angle)
    sine = jnp.sin(angle)
    sine = jnp.where(low, -sine, sine)

    arrived("tok")
    xcol[e] = tok[:, chunk(e, 256)]
    arrived("ow")
    heads_sum = to_row(jnp.sum(wo[x].astype(F32), axis=1, keepdims=True), 256, 256)
    vsend[0:1, :] = heads_sum[:, 0:128]
    vsend[1:2, :] = heads_sum[:, 128:256]
    vrecv[e] = vsend[...]

    pl.semaphore_wait(barrier, 2 * (N - 1))

    over_ep(PA, lambda a: tok.at[:, chunk(a, 256)], xcol.at[e])
    flights.append((PA, xcol.at[0:15]))

    after, ahead = 4 * y + lax.rem(x + 1, 4), 4 * y + lax.rem(x + 3, 4)
    send(PW1, wo.at[x], wo.at[x], (after, t))
    send(PW1, wo.at[x], wo.at[x], (ahead, t))
    flights.append((PW1, wo.at[0:2]))
    over_ep(PV, lambda a: vsend, vrecv.at[e])
    flights.append((PV, vrecv.at[0:15]))

    def tell(k, _):
        pl.semaphore_signal(ready, inc=1, device_id=(e, lax.rem(t + k, N)), device_id_type=MESH)
        return 0

    lax.fori_loop(1, N, tell, 0)

    arrived("qw")
    arrived("kw")
    arrived("vw")
    received(PA, xcol.at[0:15])
    bsend[...] = dot(xcol[...].reshape(256, 256), wqkv[...]).astype(BF16).reshape(N, N, 512)
    brecv[e] = bsend[e]
    over_ep(PB, lambda a: bsend.at[a], brecv.at[e])
    flights.append((PB, bsend.at[0:15]))

    received(PW1, wo.at[0:2])
    x_up, x_down = lax.rem(x + 3, 4), lax.rem(x + 1, 4)
    send(PW2, wo.at[x_up, 0:128], wo.at[x_up, 0:128], (after, t))
    send(PW2, wo.at[x_down, 128:256], wo.at[x_down, 128:256], (ahead, t))
    flights.append((PW2, wo.at[0]))

    arrived("eg")
    arrived("eu")
    arrived("dg")
    arrived("du")
    send(PWGU, wgu.at[1 - c], wgu2, partner)
    flights.append((PWGU, wgu2))
    send(PWD, wd, wd2, partner)
    flights.append((PWD, wd2))

    received(PB, brecv.at[0:15])
    qkv = jnp.sum(brecv[...].astype(F32), axis=0).astype(BF16).astype(F32)

    def rotated(v):
        swapped = jnp.where(low, pltpu.roll(v, 96, 1), pltpu.roll(v, 32, 1))
        return (v * cosine + swapped * sine).astype(BF16).astype(F32)

    first = lane < 64
    key = rotated(qkv[:, 256:384])
    value = qkv[:, 384:512]
    parts, fresh = [], jnp.zeros((1, 128), F32)
    seq = lax.broadcasted_iota(jnp.int32, (N, 128), 0)
    for sub in range(2):
        for g in range(2):
            q = rotated(qkv[:, g * 128 : (g + 1) * 128]) * 0.125
            q = jnp.where(first if sub == 0 else jnp.logical_not(first), q, 0.0)
            score = jnp.sum(q * key, axis=1, keepdims=True)
            at = lane == (2 * sub + g) * N + seq
            fresh = fresh + jnp.sum(jnp.where(at, score, 0.0), axis=0, keepdims=True)
            parts.append(q)
    turned = jnp.concatenate(parts + [jnp.zeros((64, 128), F32)], axis=0).T
    lane128 = lax.broadcasted_iota(jnp.int32, (128, 128), 1)
    for s in range(N):
        keep = (lax.rem(lane128, N) == s) & (lane128 < 64)
        qd[s * 128 : (s + 1) * 128, :] = jnp.where(keep, turned, 0.0).astype(BF16)

    arrived("lam")
    row = lax.broadcasted_iota(jnp.int32, (1, 128), 1)
    share = jnp.where(
        row < 2 * N, 1.0, jnp.where(row < 3 * N, -lam[0:1, 0:1], -lam[0:1, 1:2])
    )
    limit = jnp.sum(jnp.where(lax.rem(lane, N) == seq, length, 0), axis=0, keepdims=True)

    arrived("kc")
    scores[...] = dot(kc[...], qd[...])
    position = lax.broadcasted_iota(jnp.int32, (CACHE, 128), 0)
    masked = jnp.where(position < limit, scores[...], -1e30)
    top = jnp.maximum(jnp.max(masked, axis=0, keepdims=True), fresh)
    p = jnp.exp(masked - top)
    fresh_p = jnp.exp(fresh - top)
    scale = share / (jnp.sum(p, axis=0, keepdims=True) + fresh_p)
    p = p * scale
    fresh_p = fresh_p * scale
    p = p + pltpu.roll(p, 96, 1)
    fresh_p = jnp.broadcast_to(fresh_p, (8, 128))
    fresh_p = (fresh_p + pltpu.roll(fresh_p, 96, 1)).astype(BF16).astype(F32)[0:1, :]
    chances = p.T[0 : 2 * N, :].astype(BF16)
    arrived("vc")
    heads = dot(chances, vc[...])

    arrived("hgain")
    for g in range(2):
        weight = jnp.sum(jnp.where(lane == g * N + seq, fresh_p, 0.0), axis=1, keepdims=True)
        head = weight * value
        for s in range(N):
            head = head + jnp.where(
                seq == s, heads[g * N : (g + 1) * N, s * 128 : (s + 1) * 128], 0.0
            )
        mean = jnp.mean(head * head, axis=1, keepdims=True)
        head = head * lax.rsqrt(mean + 1e-6) * hgain[...] * 0.8
        normed[:, g * 128 : (g + 1) * 128] = head.astype(BF16)
    dnorm[y] = normed[...]

    def heads_send(k, _):
        send(PD, normed, dnorm.at[y], (4 * lax.rem(y + k, 4) + x, t))
        return 0

    lax.fori_loop(1, 4, heads_send, 0)
    flights.append((PD, dnorm.at[0:3]))
    received(PV, vrecv.at[0:15])
    weights_sum = jnp.sum(vrecv[...], axis=0)
    sums = jnp.sum(
        normed[:, 0:128].astype(F32) * weights_sum[0:1, :]
        + normed[:, 128:256].astype(F32) * weights_sum[1:2, :],
        axis=1,
        keepdims=True,
    )
    asend[...] = to_row(sums, N, 128)
    arecv[t] = asend[...]
    over_tp(PMEAN, lambda b: asend, arecv.at[t])
    flights.append((PMEAN, arecv.at[0:15]))
    pl.semaphore_wait(ready, N - 1)
    received(PW2, wo.at[0])
    received(PD, dnorm.at[0:3])

    def out_send(i, _):
        x2, y2 = i // 4, lax.rem(y + 2 + lax.rem(i, 4), 4)
        b = 4 * y + x2
        itself = (y2 == y) & (b == t)

        @pl.when(lax.rem(i, 4) == 0)
        def _():
            part = dot(dnorm[...].reshape(64, 256), wo[x2])
            esend[x2] = part.astype(BF16).reshape(4, N, 256)

        @pl.when(itself)
        def _():
            pltpu.make_async_copy(esend.at[x2, y2], erecv.at[t], rsem.at[PE]).start()

        @pl.when(jnp.logical_not(itself))
        def _():
            send(PE, esend.at[x2, y2], erecv.at[t], (4 * y2 + x, b))

        return 0

    lax.fori_loop(0, N, out_send, 0)
    flights.append((PE, erecv.at[0:15]))
    over_ep(PMETA, lambda a: meta, metas.at[e_slot])
    flights.append((PMETA, metas.at[0:15]))

    received(PMETA, metas.at[0:15])
    every = metas[...].reshape(256, 128)
    wide_lane = lax.broadcasted_iota(jnp.int32, (256, 128), 1)
    code_col = jnp.sum(jnp.where(wide_lane == e, every, 0.0), axis=1, keepdims=True)
    gate_col = jnp.sum(jnp.where(wide_lane == e + N, every, 0.0), axis=1, keepdims=True)
    block = (lax.broadcasted_iota(jnp.int32, (256, 1), 0) // N * CAP).astype(F32)
    target = jnp.where(code_col >= 0.0, code_col + block, -1.0)
    place[...] = jnp.where(
        lax.broadcasted_iota(jnp.int32, (256, 64), 1).astype(F32) == target, 1.0, 0.0
    ).astype(BF16)
    pick[...] = jnp.where(
        lax.broadcasted_iota(jnp.int32, (64, 256), 0).astype(F32) == to_row(target, 256, 256),
        1.0,
        0.0,
    ).astype(BF16)
    gates[...] = gate_col

    arrived("fgain")
    arrived("dmix")
    gw[...] = fgain[...] * dmix[...].astype(F32)

    def block_of(ref):
        return jnp.concatenate([ref[pl.ds(2 * t, 1), :], ref[pl.ds(2 * t + 1, 1), :]], axis=1)

    gain = block_of(fgain)
    gain_mix = block_of(gw)
    root = 2.0**0.5
    token_mean = root * jnp.mean(tok[...].astype(F32), axis=1, keepdims=True)
    own_tokens = root * tok[:, chunk(t, 256)].astype(F32)

    received(PE, erecv)
    residual = own_tokens + jnp.sum(erecv[...].astype(F32), axis=0)
    received(PMEAN, arecv.at[0:15])
    mean = token_mean + to_column_of(jnp.sum(arecv[...], axis=0)) * (1.0 / 4096)
    centred = residual - mean
    gsend[...] = (centred * gain).astype(BF16)
    grecv[e_slot] = gsend[...]
    over_ep(PG, lambda a: gsend, grecv.at[e_slot])
    flights.append((PG, grecv.at[0:15]))
    fsend[0:1, :] = to_row(jnp.sum(centred * centred, axis=1, keepdims=True), N, 128)
    fsend[1:2, :] = to_row(jnp.sum(centred * gain_mix, axis=1, keepdims=True), N, 128)
    frecv[t] = fsend[...]
    over_tp(PF, lambda b: fsend, frecv.at[t])
    flights.append((PF, frecv.at[0:15]))

    received(PG, grecv.at[0:15])
    xsend[...] = dot(pick[...], grecv[...].reshape(256, 256)).astype(BF16)
    send(PX, xsend, xrecv, partner)
    flights.append((PX, xrecv))
    send(PXR, grecv.at[pl.ds((1 - c) * 8, 8)], xrows, partner)
    flights.append((PXR, xrows))

    received(PWGU, wgu2)
    received(PWD, wd2)
    received(PX, xrecv)
    received(PXR, xrows)
    mine = grecv[pl.ds(c * 8, 8)].reshape(128, 256)
    dense_pre = dot(mine, wd[...]) + dot(xrows[...].reshape(128, 256), wd2[...])
    hsend[:, 64:80, :] = dense_pre.astype(BF16).reshape(8, N, 256)

    def partial(chip):
        cols = chunk(chip, 256)
        pre = dot(xsend[...], wgu[c, :, cols]) + dot(xrecv[...], wgu2[:, cols])
        hsend[chip, 0:64, :] = pre.astype(BF16)

    def project(i, _):
        chip = lax.rem(z + far_first(i, 8), 8)
        partial(chip)
        send(PH, hsend.at[chip], hrecv.at[z], (e, 2 * chip + c))
        return 0

    lax.fori_loop(0, 7, project, 0)
    flights.append((PH, hsend.at[0:7]))
    partial(z)
    hrecv[z] = hsend[z]

    received(PF, frecv.at[0:15])
    totals = jnp.sum(frecv[...], axis=0)
    scale_row = lax.rsqrt(totals[0:1, :] * (1.0 / 4096) + 1e-5)
    mix = 1.0 / (1.0 + jnp.exp(-scale_row * totals[1:2, :]))
    ssend[0:1, :] = scale_row
    ssend[1:2, :] = mix
    srecv[e_slot] = ssend[...]
    over_ep(PS, lambda a: ssend, srecv.at[e_slot])
    flights.append((PS, srecv.at[0:15]))

    received(PS, srecv.at[0:15])
    own = lax.broadcasted_iota(jnp.int32, (N, N, 128), 1) == lax.broadcasted_iota(
        jnp.int32, (N, N, 128), 2
    )

    def token_column(rows):
        spread = jnp.where(own, jnp.broadcast_to(rows, (N, N, 128)), 0.0)
        return jnp.sum(spread, axis=2, keepdims=True).reshape(256, 1)

    mix_col = token_column(srecv[:, 1:2, :])
    scale_col = token_column(srecv[:, 0:1, :])
    row_scale = to_column(
        jnp.sum(jnp.where(place[...].astype(F32) > 0.5, scale_col, 0.0), axis=0, keepdims=True), 64
    )
    dense_scale = to_column_of(srecv[slot_of(t), 0:1, :])
    all_scale = jnp.concatenate([row_scale, dense_scale], axis=0)
    hidden = centred * to_column_of(scale_row) * gain

    received(PH, hrecv.at[0:7])
    pre = jnp.sum(hrecv[...].astype(F32), axis=0) * all_scale
    pre_gate = pre[:, 0:128]
    active = (pre_gate / (1.0 + jnp.exp(-pre_gate)) * pre[:, 128:256]).astype(BF16)
    isend[...] = active[0:64, :]
    idsend[...] = active[64:80, :]
    ihid[c, :, chunk(z, 128)] = isend[...]
    idense[c * 8 + z] = idsend[...]
    over_z(PI, lambda chip: isend, ihid.at[c, :, chunk(z, 128)])
    flights.append((PI, ihid.at[0, :, 0 : 7 * 128]))
    over_z(PID, lambda chip: idsend, idense.at[c * 8 + z])
    flights.append((PID, idense.at[0:7]))
    arrived("ed")
    arrived("dd")
    received(PI, ihid.at[0, :, 0 : 7 * 128])
    send(PC, ihid.at[c], ihid.at[c], partner)
    flights.append((PC, ihid.at[0]))
    received(PID, idense.at[0:7])
    send(PCD, idense.at[pl.ds(c * 8, 8)], idense.at[pl.ds(c * 8, 8)], partner)
    flights.append((PCD, idense.at[0:8]))
    result = dot(ihid[c], ed[c])
    received(PC, ihid.at[0])
    received(PCD, idense.at[0:8])
    result = (result + dot(ihid[1 - c], ed[1 - c])).astype(BF16)
    dense = dot(idense[...].reshape(256, 128), dd[...]) * mix_col
    mixture = dot(place[...], result) * gates[...] + dense
    jsend[...] = mixture.astype(BF16).reshape(N, N, 256)
    jrecv[e] = jsend[e_slot]
    over_ep(PJ, lambda a: jsend.at[slot_of(a)], jrecv.at[e])
    flights.append((PJ, jsend.at[0:15]))
    arrived("sgain")
    received(PJ, jrecv.at[0:15])
    combined = root * hidden.astype(BF16).astype(F32) + jnp.sum(jrecv[...].astype(F32), axis=0)

    mean_b = jnp.sum(combined, axis=1, keepdims=True) * (1.0 / 256)
    apart = combined - mean_b
    ksend[0:1, :] = to_row(mean_b, N, 128)
    ksend[1:2, :] = to_row(jnp.sum(apart * apart, axis=1, keepdims=True), N, 128)
    krecv[t] = ksend[...]
    over_tp(PK, lambda b: ksend, krecv.at[t])
    flights.append((PK, krecv.at[0:15]))
    received(PK, krecv.at[0:15])
    means = krecv[:, 0, :]
    mean = jnp.sum(means, axis=0, keepdims=True) * (1.0 / N)
    off = means - mean
    square = jnp.sum(krecv[:, 1, :] + 256.0 * off * off, axis=0, keepdims=True)
    scale = lax.rsqrt(square * (1.0 / 4096) + 1e-5)
    last_gain = jnp.concatenate([sgain[0:1, :], sgain[1:2, :]], axis=1)
    out_ref[...] = (
        (combined - to_column_of(mean)) * to_column_of(scale) * last_gain
    ).astype(BF16)

    for phase, blocks in flights:
        sent(phase, blocks)

    if any(phase == PE for phase, _ in flights):

        @pl.when(t // 4 != y)
        def _():
            sent(PE, erecv.at[0])


def to_column_of(row):
    same = lax.broadcasted_iota(jnp.int32, (N, 128), 0) == lax.broadcasted_iota(
        jnp.int32, (N, 128), 1
    )
    return jnp.sum(jnp.where(same, jnp.broadcast_to(row, (N, 128)), 0), axis=1, keepdims=True)


def on_device(
    tokens, query_weight, key_weight, value_weight, out_weight, head_lambda, head_gain,
    key_cache, value_cache, lengths, first_gain, second_gain, expert_ids, route_weights,
    expert_gate, expert_up, expert_down, dense_gate, dense_up, dense_down, dense_mix,
):
    anywhere = pl.BlockSpec(memory_space=pltpu.HBM)
    vmem = pltpu.VMEM
    scratch = [
        vmem((N, 4096), BF16),
        vmem((256, 512), BF16),
        vmem((4, 256, 256), BF16),
        vmem((1, 2), F32),
        vmem((1, 128), F32),
        vmem((CACHE, N * 128), BF16),
        vmem((CACHE, N * 128), BF16),
        vmem((1, N), jnp.int32),
        vmem((32, 128), F32),
        vmem((2, 128), F32),
        vmem((2, N), jnp.int32),
        vmem((2, N), F32),
        vmem((2, 256, 2048), BF16),
        vmem((256, 2048), BF16),
        vmem((2, 1024, 256), BF16),
        vmem((256, 256), BF16),
        vmem((256, 256), BF16),
        vmem((128, 256), BF16),
        vmem((32, 128), BF16),
        vmem((N, N, 256), BF16),
        vmem((N, 128), F32),
        vmem((N, N, 128), F32),
        vmem((N, N, 512), BF16),
        vmem((N, N, 512), BF16),
        vmem((N * 128, 128), BF16),
        vmem((CACHE, 128), F32),
        vmem((N, 256), BF16),
        vmem((4, N, 256), BF16),
        vmem((2, 128), F32),
        vmem((N, 2, 128), F32),
        vmem((4, 4, N, 256), BF16),
        vmem((N, N, 256), BF16),
        vmem((1, 128), F32),
        vmem((N, 1, 128), F32),
        vmem((2, 128), F32),
        vmem((N, 2, 128), F32),
        vmem((N, 256), BF16),
        vmem((N, N, 256), BF16),
        vmem((2, 128), F32),
        vmem((N, 2, 128), F32),
        vmem((32, 128), F32),
        vmem((64, 256), BF16),
        vmem((64, 256), BF16),
        vmem((8, N, 256), BF16),
        vmem((8, 80, 256), BF16),
        vmem((8, 80, 256), BF16),
        vmem((64, 128), BF16),
        vmem((N, 128), BF16),
        vmem((2, 64, 1024), BF16),
        vmem((N, N, 128), BF16),
        vmem((N, N, 256), BF16),
        vmem((N, N, 256), BF16),
        vmem((2, 128), F32),
        vmem((N, 2, 128), F32),
        vmem((64, 256), BF16),
        vmem((256, 64), BF16),
        vmem((256, 1), F32),
        pltpu.SemaphoreType.DMA((len(LOCALS),)),
        pltpu.SemaphoreType.DMA((PHASES,)),
        pltpu.SemaphoreType.DMA((PHASES,)),
        pltpu.SemaphoreType.REGULAR,
    ]
    return pl.pallas_call(
        kernel,
        out_shape=jax.ShapeDtypeStruct((N, 256), BF16),
        in_specs=[anywhere] * 21,
        out_specs=pl.BlockSpec(memory_space=pltpu.VMEM),
        scratch_shapes=scratch,
        compiler_params=pltpu.CompilerParams(
            collective_id=0, has_side_effects=True, vmem_limit_bytes=67_043_328
        ),
        name="layer",
    )(
        tokens,
        query_weight,
        key_weight,
        value_weight,
        out_weight,
        head_lambda.reshape(1, 2),
        head_gain.reshape(1, 128),
        key_cache.reshape(N, CACHE, 128),
        value_cache.reshape(N, CACHE, 128),
        lengths.reshape(1, N),
        first_gain.reshape(32, 128),
        second_gain.reshape(2, 128),
        expert_ids.T,
        route_weights.T,
        expert_gate.reshape(256, 2048),
        expert_up.reshape(256, 2048),
        expert_down.reshape(2048, 256),
        dense_gate,
        dense_up,
        dense_down,
        dense_mix.reshape(32, 128),
    )


def solution(mesh):
    return jax.shard_map(
        on_device,
        mesh=mesh,
        in_specs=(
            P("ep", None),
            P("ep", "tp"),
            P("ep", "tp"),
            P("ep", "tp"),
            P("tp", "ep"),
            P("tp"),
            P(),
            P("ep", None, "tp", None),
            P("ep", None, "tp", None),
            P("ep"),
            P(),
            P("tp"),
            P("ep", None),
            P("ep", None),
            P("ep", "tp", None),
            P("ep", "tp", None),
            P("ep", None, "tp"),
            P("tp", "ep"),
            P("tp", "ep"),
            P("ep", "tp"),
            P(),
        ),
        out_specs=P("ep", "tp"),
        check_vma=False,
    )
```

```python
import functools
import math

import jax
import jax.numpy as jnp
from jax import lax
from jax.experimental import pallas as pl
from jax.experimental.pallas import tpu as pltpu
from jax.sharding import PartitionSpec as P

N = 16
CACHE = 1024
CAP = 4
F32 = jnp.float32
BF16 = jnp.bfloat16
MESH = pl.DeviceIdType.MESH

(
    PA, PMETA, PB, PV, PW1, PW2, PWGU, PWD, PD, PE, PMEAN, PF, PG, PS, PX, PXR, PH, PI, PID, PC, PCD, PJ, PK,
) = range(23)
PHASES = 23

LOCALS = (
    "tok", "qw", "kw", "vw", "ow", "lam", "hgain", "kc", "vc", "lens", "fgain",
    "sgain", "ids", "rw", "eg", "eu", "ed", "dg", "du", "dd", "dmix",
)


def dot(a, b):
    return jnp.dot(a, b, preferred_element_type=F32)


def to_column(row, n):
    same = lax.broadcasted_iota(jnp.int32, (n, n), 0) == lax.broadcasted_iota(jnp.int32, (n, n), 1)
    return jnp.sum(jnp.where(same, jnp.broadcast_to(row, (n, n)), 0), axis=1, keepdims=True)


def to_row(column, n, lanes):
    same = lax.broadcasted_iota(jnp.int32, (n, lanes), 0) == lax.broadcasted_iota(
        jnp.int32, (n, lanes), 1
    )
    return jnp.sum(jnp.where(same, jnp.broadcast_to(column, (n, lanes)), 0), axis=0, keepdims=True)


def slot_of(i):
    return lax.rem(i, 2) * 8 + i // 2


def kernel(
    tok_h, qw_h, kw_h, vw_h, ow_h, lam_h, hgain_h, kc_h, vc_h, lens_h, fgain_h, sgain_h,
    ids_h, rw_h, eg_h, eu_h, ed_h, dg_h, du_h, dd_h, dmix_h,
    out_ref,
    tok, wqkv, wown, wo, lam, hgain, kc, vc, lens, fgain, sgain, ids, rw, wgu, wgu2, ed, wd, wd2, dd, dmix,
    xcol, meta, metas, bsend, brecv, qd, scores, normed, dnorm, vsend, vrecv, esend, erecv,
    asend, arecv, fsend, frecv, gsend, grecv, ssend, srecv, gw, xsend, xrecv, xrows,
    hsend, hrecv, isend, idsend, ihid, idense,
    jsend, jrecv, ksend, krecv, pick, place, gates,
    lsem, ssem, rsem, ready,
):
    e = lax.axis_index("ep")
    t = lax.axis_index("tp")
    z, c = t // 2, lax.rem(t, 2)
    partner = (e, 2 * z + 1 - c)
    y, x = e // 4, lax.rem(e, 4)
    e_slot = slot_of(e)

    def chunk(i, width):
        return pl.ds(pl.multiple_of(i * width, width), width)

    barrier = pltpu.get_barrier_semaphore()

    def greet(k, _):
        pl.semaphore_signal(
            barrier, inc=1, device_id=(lax.rem(e + k, N), t), device_id_type=MESH
        )
        pl.semaphore_signal(
            barrier, inc=1, device_id=(e, lax.rem(t + k, N)), device_id_type=MESH
        )
        return 0

    lax.fori_loop(1, N, greet, 0)

    coming, flights = {}, []

    def bring(name, pairs, whole=None):
        sem = lsem.at[LOCALS.index(name)]
        coming[name] = pairs[0][1] if whole is None else whole
        for src, dst in pairs:
            pltpu.make_async_copy(src, dst, sem).start()

    def arrived(name):
        whole = coming.pop(name)
        pltpu.make_async_copy(whole, whole, lsem.at[LOCALS.index(name)]).wait()

    bring("tok", [(tok_h, tok)])
    bring("ids", [(ids_h, ids)])
    bring("rw", [(rw_h, rw)])
    bring("ow", [(ow_h, wown)])
    bring("qw", [(qw_h, wqkv.at[:, 0:256])])
    bring("kw", [(kw_h, wqkv.at[:, 256:384])])
    bring("vw", [(vw_h, wqkv.at[:, 384:512])])
    bring("lens", [(lens_h, lens)])
    bring("lam", [(lam_h, lam)])
    bring("hgain", [(hgain_h, hgain)])
    bring("fgain", [(fgain_h, fgain)])
    bring("dmix", [(dmix_h, dmix)])
    bring("sgain", [(sgain_h, sgain)])

    def bring_pair(i, _):
        sem_g = lsem.at[LOCALS.index("eg")]
        sem_u = lsem.at[LOCALS.index("eu")]
        core, chip = lax.rem(i, 2), i // 2
        even = pl.ds(pl.multiple_of(chip * 256, 256), 128)
        odd = pl.ds(pl.multiple_of(chip * 256 + 128, 128), 128)
        pltpu.make_async_copy(eg_h.at[:, chunk(i, 128)], wgu.at[core, :, even], sem_g).start()
        pltpu.make_async_copy(eu_h.at[:, chunk(i, 128)], wgu.at[core, :, odd], sem_u).start()
        return 0

    lax.fori_loop(0, N, bring_pair, 0)
    coming["eg"] = wgu.at[0]
    coming["eu"] = wgu.at[1]
    bring("dg", [(dg_h, wd.at[:, 0:128])])
    bring("du", [(du_h, wd.at[:, 128:256])])
    bring("kc", [(kc_h.at[s], kc.at[:, s * 128 : (s + 1) * 128]) for s in range(N)], kc)
    bring("vc", [(vc_h.at[s], vc.at[:, s * 128 : (s + 1) * 128]) for s in range(N)], vc)

    def bring_down(i, _):
        core, chip = lax.rem(i, 2), i // 2
        pltpu.make_async_copy(
            ed_h.at[chunk(i, 128), :], ed.at[core, chunk(chip, 128), :], lsem.at[LOCALS.index("ed")]
        ).start()
        return 0

    lax.fori_loop(0, N, bring_down, 0)
    coming["ed"] = ed
    bring("dd", [(dd_h, dd)])

    def send(phase, src, dst, to):
        pltpu.make_async_remote_copy(
            src_ref=src,
            dst_ref=dst,
            send_sem=ssem.at[phase],
            recv_sem=rsem.at[phase],
            device_id=to,
            device_id_type=MESH,
        ).start()

    def over_ep(phase, src_of, dst):
        def one(k, _):
            a = lax.rem(e + k, N)
            send(phase, src_of(a), dst, (a, t))
            return 0

        lax.fori_loop(1, N, one, 0)

    def far_first(i, n):
        half = (i + 1) // 2
        return n // 2 + half * (2 * lax.rem(i + 1, 2) - 1)

    def over_tp(phase, src_of, dst):
        def one(i, _):
            b = lax.rem(t + far_first(i, N), N)
            send(phase, src_of(b), dst, (e, b))
            return 0

        lax.fori_loop(0, N - 1, one, 0)

    def over_z(phase, src_of, dst):
        def one(i, _):
            chip = lax.rem(z + far_first(i, 8), 8)
            send(phase, src_of(chip), dst, (e, 2 * chip + c))
            return 0

        lax.fori_loop(0, 7, one, 0)

    def received(phase, blocks):
        pltpu.make_async_copy(blocks, blocks, rsem.at[phase]).wait()

    def sent(phase, blocks):
        pltpu.make_async_copy(blocks, blocks, ssem.at[phase]).wait()

    lane = lax.broadcasted_iota(jnp.int32, (N, 128), 1)

    arrived("ids")
    arrived("rw")
    id0 = to_column(ids[0:1, :], N)
    id1 = to_column(ids[1:2, :], N)
    w0 = to_column(rw[0:1, :], N)
    w1 = to_column(rw[1:2, :], N)
    total = w0 + w1
    hit0 = lane == id0
    hit1 = lane == id1
    hit = jnp.where(hit0 | hit1, 1.0, 0.0).astype(F32)
    before = jnp.where(
        lax.broadcasted_iota(jnp.int32, (N, N), 1) < lax.broadcasted_iota(jnp.int32, (N, N), 0),
        1.0,
        0.0,
    ).astype(F32)
    slot = dot(before.astype(BF16), hit.astype(BF16))
    code = jnp.where(hit > 0.5, slot, -1.0)
    gate0 = jnp.where(lane - N == id0, w0 / total, 0.0)
    gate1 = jnp.where(lane - N == id1, w1 / total, 0.0)
    meta[...] = jnp.where(lane < N, code, gate0 + gate1)
    metas[e_slot] = meta[...]

    arrived("lens")
    length = to_column(lens[...], N)
    turn = lax.rem(lane, 32).astype(F32) * (2.0 / 64)
    angle = length.astype(F32) * jnp.exp(turn * (-math.log(500000.0)))
    low = lax.rem(lane, 64) < 32
    cosine = jnp.cos(angle)
    sine = jnp.sin(angle)
    sine = jnp.where(low, -sine, sine)

    arrived("tok")
    xcol[e] = tok[:, chunk(e, 256)]
    arrived("ow")
    heads_sum = to_row(jnp.sum(wown[...].astype(F32), axis=1, keepdims=True), 256, 256)
    vsend[0:1, :] = heads_sum[:, 0:128]
    vsend[1:2, :] = heads_sum[:, 128:256]
    vrecv[e] = vsend[...]

    pl.semaphore_wait(barrier, 2 * (N - 1))

    over_ep(PA, lambda a: tok.at[:, chunk(a, 256)], xcol.at[e])
    flights.append((PA, xcol.at[0:15]))

    def tell(k, _):
        pl.semaphore_signal(ready, inc=1, device_id=(e, lax.rem(t + k, N)), device_id_type=MESH)
        return 0

    lax.fori_loop(1, N, tell, 0)

    arrived("qw")
    arrived("kw")
    arrived("vw")
    received(PA, xcol.at[0:15])
    bsend[...] = dot(xcol[...].reshape(256, 256), wqkv[...]).astype(BF16).reshape(N, N, 512)
    brecv[e] = bsend[e]
    over_ep(PB, lambda a: bsend.at[a], brecv.at[e])
    flights.append((PB, bsend.at[0:15]))

    after, ahead = 4 * y + lax.rem(x + 1, 4), 4 * y + lax.rem(x + 3, 4)
    goal = lax.rem(x, 2)
    same = goal == c
    other = jnp.logical_not(same)
    landing = wo.at[x // 2, chunk(c, 256)]
    send(PW1, wown, landing, (after, 2 * z + goal))
    send(PW1, wown, landing, (ahead, 2 * z + goal))

    @pl.when(same)
    def _():
        pltpu.make_async_copy(wown, landing, rsem.at[PW1]).start()

    @pl.when(other)
    def _():
        send(PW1, wown, landing, partner)

    flights.append((PW1, wo.at[0]))
    over_ep(PV, lambda a: vsend, vrecv.at[e])
    flights.append((PV, vrecv.at[0:15]))

    arrived("eg")
    arrived("eu")
    arrived("dg")
    arrived("du")
    send(PWGU, wgu.at[1 - c], wgu2, partner)
    flights.append((PWGU, wgu2))
    send(PWD, wd, wd2, partner)
    flights.append((PWD, wd2))

    received(PB, brecv.at[0:15])
    qkv = jnp.sum(brecv[...].astype(F32), axis=0).astype(BF16).astype(F32)

    def rotated(v):
        swapped = jnp.where(low, pltpu.roll(v, 96, 1), pltpu.roll(v, 32, 1))
        return (v * cosine + swapped * sine).astype(BF16).astype(F32)

    first = lane < 64
    key = rotated(qkv[:, 256:384])
    value = qkv[:, 384:512]
    parts, fresh = [], jnp.zeros((1, 128), F32)
    seq = lax.broadcasted_iota(jnp.int32, (N, 128), 0)
    for sub in range(2):
        for g in range(2):
            q = rotated(qkv[:, g * 128 : (g + 1) * 128]) * 0.125
            q = jnp.where(first if sub == 0 else jnp.logical_not(first), q, 0.0)
            score = jnp.sum(q * key, axis=1, keepdims=True)
            at = lane == (2 * sub + g) * N + seq
            fresh = fresh + jnp.sum(jnp.where(at, score, 0.0), axis=0, keepdims=True)
            parts.append(q)
    turned = jnp.concatenate(parts + [jnp.zeros((64, 128), F32)], axis=0).T
    lane128 = lax.broadcasted_iota(jnp.int32, (128, 128), 1)
    for s in range(N):
        keep = (lax.rem(lane128, N) == s) & (lane128 < 64)
        qd[s * 128 : (s + 1) * 128, :] = jnp.where(keep, turned, 0.0).astype(BF16)

    arrived("lam")
    row = lax.broadcasted_iota(jnp.int32, (1, 128), 1)
    share = jnp.where(
        row < 2 * N, 1.0, jnp.where(row < 3 * N, -lam[0:1, 0:1], -lam[0:1, 1:2])
    )
    limit = jnp.sum(jnp.where(lax.rem(lane, N) == seq, length, 0), axis=0, keepdims=True)

    arrived("kc")
    scores[...] = dot(kc[...], qd[...])
    position = lax.broadcasted_iota(jnp.int32, (CACHE, 128), 0)
    masked = jnp.where(position < limit, scores[...], -1e30)
    top = jnp.maximum(jnp.max(masked, axis=0, keepdims=True), fresh)
    p = jnp.exp(masked - top)
    fresh_p = jnp.exp(fresh - top)
    scale = share / (jnp.sum(p, axis=0, keepdims=True) + fresh_p)
    p = p * scale
    fresh_p = fresh_p * scale
    p = p + pltpu.roll(p, 96, 1)
    fresh_p = jnp.broadcast_to(fresh_p, (8, 128))
    fresh_p = (fresh_p + pltpu.roll(fresh_p, 96, 1)).astype(BF16).astype(F32)[0:1, :]
    chances = p.T[0 : 2 * N, :].astype(BF16)
    arrived("vc")
    @pl.when(same)
    def _():
        received(PW1, wo.at[0])

    @pl.when(other)
    def _():
        received(PW1, wo)
        x_up, x_down = lax.rem(x + 3, 4), lax.rem(x + 1, 4)
        low_half, high_half = wo.at[x_down // 2, 0:256], wo.at[x_up // 2, 256:512]
        send(PW2, low_half, low_half, (ahead, t))
        send(PW2, high_half, high_half, (after, t))

    heads = dot(chances, vc[...])

    arrived("hgain")
    for g in range(2):
        weight = jnp.sum(jnp.where(lane == g * N + seq, fresh_p, 0.0), axis=1, keepdims=True)
        head = weight * value
        for s in range(N):
            head = head + jnp.where(
                seq == s, heads[g * N : (g + 1) * N, s * 128 : (s + 1) * 128], 0.0
            )
        mean = jnp.mean(head * head, axis=1, keepdims=True)
        head = head * lax.rsqrt(mean + 1e-6) * hgain[...] * 0.8
        normed[:, g * 128 : (g + 1) * 128] = head.astype(BF16)
    pl.semaphore_wait(ready, N - 1)
    dnorm[c * 4 + y] = normed[...]

    def heads_send(k, _):
        e2 = 4 * lax.rem(y + k, 4) + x
        send(PD, normed, dnorm.at[c * 4 + y], (e2, t))
        send(PD, normed, dnorm.at[c * 4 + y], (e2, 2 * z + 1 - c))
        return 0

    lax.fori_loop(1, 4, heads_send, 0)
    send(PD, normed, dnorm.at[c * 4 + y], partner)
    flights.append((PD, dnorm.at[0:7]))
    received(PV, vrecv.at[0:15])
    weights_sum = jnp.sum(vrecv[...], axis=0)
    sums = jnp.sum(
        normed[:, 0:128].astype(F32) * weights_sum[0:1, :]
        + normed[:, 128:256].astype(F32) * weights_sum[1:2, :],
        axis=1,
        keepdims=True,
    )
    asend[...] = to_row(sums, N, 128)
    arecv[t] = asend[...]
    over_tp(PMEAN, lambda b: asend, arecv.at[t])
    flights.append((PMEAN, arecv.at[0:15]))

    @pl.when(same)
    def _():
        received(PW2, wo.at[0])

    received(PD, dnorm.at[0:7])

    def out_send(i, _):
        j, y2 = i // 4, lax.rem(y + 2 + lax.rem(i, 4), 4)
        b = 4 * y + 2 * j + c
        itself = (y2 == y) & (b == t)

        @pl.when(lax.rem(i, 4) == 0)
        def _():
            part = dot(dnorm[0:4].reshape(64, 256), wo[j, 0:256])
            part = part + dot(dnorm[4:8].reshape(64, 256), wo[j, 256:512])
            esend[j] = part.astype(BF16).reshape(4, N, 256)

        @pl.when(itself)
        def _():
            pltpu.make_async_copy(esend.at[j, y2], erecv.at[z], rsem.at[PE]).start()

        @pl.when(jnp.logical_not(itself))
        def _():
            send(PE, esend.at[j, y2], erecv.at[z], (4 * y2 + x, b))

        return 0

    lax.fori_loop(0, 8, out_send, 0)
    flights.append((PE, erecv.at[0:7]))
    over_ep(PMETA, lambda a: meta, metas.at[e_slot])
    flights.append((PMETA, metas.at[0:15]))

    received(PMETA, metas.at[0:15])
    every = metas[...].reshape(256, 128)
    wide_lane = lax.broadcasted_iota(jnp.int32, (256, 128), 1)
    code_col = jnp.sum(jnp.where(wide_lane == e, every, 0.0), axis=1, keepdims=True)
    gate_col = jnp.sum(jnp.where(wide_lane == e + N, every, 0.0), axis=1, keepdims=True)
    block = (lax.broadcasted_iota(jnp.int32, (256, 1), 0) // N * CAP).astype(F32)
    target = jnp.where(code_col >= 0.0, code_col + block, -1.0)
    place[...] = jnp.where(
        lax.broadcasted_iota(jnp.int32, (256, 64), 1).astype(F32) == target, 1.0, 0.0
    ).astype(BF16)
    pick[...] = jnp.where(
        lax.broadcasted_iota(jnp.int32, (64, 256), 0).astype(F32) == to_row(target, 256, 256),
        1.0,
        0.0,
    ).astype(BF16)
    gates[...] = gate_col

    arrived("fgain")
    arrived("dmix")
    gw[...] = fgain[...] * dmix[...].astype(F32)

    def block_of(ref):
        return jnp.concatenate([ref[pl.ds(2 * t, 1), :], ref[pl.ds(2 * t + 1, 1), :]], axis=1)

    gain = block_of(fgain)
    gain_mix = block_of(gw)
    root = 2.0**0.5
    token_mean = root * jnp.mean(tok[...].astype(F32), axis=1, keepdims=True)
    own_tokens = root * tok[:, chunk(t, 256)].astype(F32)

    received(PE, erecv)
    residual = own_tokens + jnp.sum(erecv[...].astype(F32), axis=0)
    received(PMEAN, arecv.at[0:15])
    mean = token_mean + to_column_of(jnp.sum(arecv[...], axis=0)) * (1.0 / 4096)
    centred = residual - mean
    gsend[...] = (centred * gain).astype(BF16)
    grecv[e_slot] = gsend[...]
    over_ep(PG, lambda a: gsend, grecv.at[e_slot])
    flights.append((PG, grecv.at[0:15]))
    fsend[0:1, :] = to_row(jnp.sum(centred * centred, axis=1, keepdims=True), N, 128)
    fsend[1:2, :] = to_row(jnp.sum(centred * gain_mix, axis=1, keepdims=True), N, 128)
    frecv[t] = fsend[...]
    over_tp(PF, lambda b: fsend, frecv.at[t])
    flights.append((PF, frecv.at[0:15]))

    received(PG, grecv.at[0:15])
    xsend[...] = dot(pick[...], grecv[...].reshape(256, 256)).astype(BF16)
    send(PX, xsend, xrecv, partner)
    flights.append((PX, xrecv))
    send(PXR, grecv.at[pl.ds((1 - c) * 8, 8)], xrows, partner)
    flights.append((PXR, xrows))

    received(PWGU, wgu2)
    received(PWD, wd2)
    received(PX, xrecv)
    received(PXR, xrows)
    mine = grecv[pl.ds(c * 8, 8)].reshape(128, 256)
    dense_pre = dot(mine, wd[...]) + dot(xrows[...].reshape(128, 256), wd2[...])
    hsend[:, 64:80, :] = dense_pre.astype(BF16).reshape(8, N, 256)

    def partial(chip):
        cols = chunk(chip, 256)
        pre = dot(xsend[...], wgu[c, :, cols]) + dot(xrecv[...], wgu2[:, cols])
        hsend[chip, 0:64, :] = pre.astype(BF16)

    def project(i, _):
        chip = lax.rem(z + far_first(i, 8), 8)
        partial(chip)
        send(PH, hsend.at[chip], hrecv.at[z], (e, 2 * chip + c))
        return 0

    lax.fori_loop(0, 7, project, 0)
    flights.append((PH, hsend.at[0:7]))
    partial(z)
    hrecv[z] = hsend[z]

    received(PF, frecv.at[0:15])
    totals = jnp.sum(frecv[...], axis=0)
    scale_row = lax.rsqrt(totals[0:1, :] * (1.0 / 4096) + 1e-5)
    mix = 1.0 / (1.0 + jnp.exp(-scale_row * totals[1:2, :]))
    ssend[0:1, :] = scale_row
    ssend[1:2, :] = mix
    srecv[e_slot] = ssend[...]
    over_ep(PS, lambda a: ssend, srecv.at[e_slot])
    flights.append((PS, srecv.at[0:15]))

    received(PS, srecv.at[0:15])
    own = lax.broadcasted_iota(jnp.int32, (N, N, 128), 1) == lax.broadcasted_iota(
        jnp.int32, (N, N, 128), 2
    )

    def token_column(rows):
        spread = jnp.where(own, jnp.broadcast_to(rows, (N, N, 128)), 0.0)
        return jnp.sum(spread, axis=2, keepdims=True).reshape(256, 1)

    mix_col = token_column(srecv[:, 1:2, :])
    scale_col = token_column(srecv[:, 0:1, :])
    row_scale = to_column(
        jnp.sum(jnp.where(place[...].astype(F32) > 0.5, scale_col, 0.0), axis=0, keepdims=True), 64
    )
    dense_scale = to_column_of(srecv[slot_of(t), 0:1, :])
    all_scale = jnp.concatenate([row_scale, dense_scale], axis=0)
    hidden = centred * to_column_of(scale_row) * gain

    received(PH, hrecv.at[0:7])
    pre = jnp.sum(hrecv[...].astype(F32), axis=0) * all_scale
    pre_gate = pre[:, 0:128]
    active = (pre_gate / (1.0 + jnp.exp(-pre_gate)) * pre[:, 128:256]).astype(BF16)
    isend[...] = active[0:64, :]
    idsend[...] = active[64:80, :]
    ihid[c, :, chunk(z, 128)] = isend[...]
    idense[c * 8 + z] = idsend[...]
    over_z(PI, lambda chip: isend, ihid.at[c, :, chunk(z, 128)])
    flights.append((PI, ihid.at[0, :, 0 : 7 * 128]))
    over_z(PID, lambda chip: idsend, idense.at[c * 8 + z])
    flights.append((PID, idense.at[0:7]))
    arrived("ed")
    arrived("dd")
    received(PI, ihid.at[0, :, 0 : 7 * 128])
    send(PC, ihid.at[c], ihid.at[c], partner)
    flights.append((PC, ihid.at[0]))
    received(PID, idense.at[0:7])
    send(PCD, idense.at[pl.ds(c * 8, 8)], idense.at[pl.ds(c * 8, 8)], partner)
    flights.append((PCD, idense.at[0:8]))
    result = dot(ihid[c], ed[c])
    received(PC, ihid.at[0])
    received(PCD, idense.at[0:8])
    result = (result + dot(ihid[1 - c], ed[1 - c])).astype(BF16)
    dense = dot(idense[...].reshape(256, 128), dd[...]) * mix_col
    mixture = dot(place[...], result) * gates[...] + dense
    jsend[...] = mixture.astype(BF16).reshape(N, N, 256)
    jrecv[e] = jsend[e_slot]
    over_ep(PJ, lambda a: jsend.at[slot_of(a)], jrecv.at[e])
    flights.append((PJ, jsend.at[0:15]))
    arrived("sgain")
    received(PJ, jrecv.at[0:15])
    combined = root * hidden.astype(BF16).astype(F32) + jnp.sum(jrecv[...].astype(F32), axis=0)

    mean_b = jnp.sum(combined, axis=1, keepdims=True) * (1.0 / 256)
    apart = combined - mean_b
    ksend[0:1, :] = to_row(mean_b, N, 128)
    ksend[1:2, :] = to_row(jnp.sum(apart * apart, axis=1, keepdims=True), N, 128)
    krecv[t] = ksend[...]
    over_tp(PK, lambda b: ksend, krecv.at[t])
    flights.append((PK, krecv.at[0:15]))
    received(PK, krecv.at[0:15])
    means = krecv[:, 0, :]
    mean = jnp.sum(means, axis=0, keepdims=True) * (1.0 / N)
    off = means - mean
    square = jnp.sum(krecv[:, 1, :] + 256.0 * off * off, axis=0, keepdims=True)
    scale = lax.rsqrt(square * (1.0 / 4096) + 1e-5)
    last_gain = jnp.concatenate([sgain[0:1, :], sgain[1:2, :]], axis=1)
    out_ref[...] = (
        (combined - to_column_of(mean)) * to_column_of(scale) * last_gain
    ).astype(BF16)

    for phase, blocks in flights:
        sent(phase, blocks)

    @pl.when(other)
    def _():
        sent(PW1, wown)
        sent(PW2, wo.at[0])

    if any(phase == PE for phase, _ in flights):

        @pl.when(t // 4 != y)
        def _():
            sent(PE, erecv.at[0])


def to_column_of(row):
    same = lax.broadcasted_iota(jnp.int32, (N, 128), 0) == lax.broadcasted_iota(
        jnp.int32, (N, 128), 1
    )
    return jnp.sum(jnp.where(same, jnp.broadcast_to(row, (N, 128)), 0), axis=1, keepdims=True)


def on_device(
    tokens, query_weight, key_weight, value_weight, out_weight, head_lambda, head_gain,
    key_cache, value_cache, lengths, first_gain, second_gain, expert_ids, route_weights,
    expert_gate, expert_up, expert_down, dense_gate, dense_up, dense_down, dense_mix,
):
    anywhere = pl.BlockSpec(memory_space=pltpu.HBM)
    vmem = pltpu.VMEM
    scratch = [
        vmem((N, 4096), BF16),
        vmem((256, 512), BF16),
        vmem((256, 256), BF16),
        vmem((2, 512, 256), BF16),
        vmem((1, 2), F32),
        vmem((1, 128), F32),
        vmem((CACHE, N * 128), BF16),
        vmem((CACHE, N * 128), BF16),
        vmem((1, N), jnp.int32),
        vmem((32, 128), F32),
        vmem((2, 128), F32),
        vmem((2, N), jnp.int32),
        vmem((2, N), F32),
        vmem((2, 256, 2048), BF16),
        vmem((256, 2048), BF16),
        vmem((2, 1024, 256), BF16),
        vmem((256, 256), BF16),
        vmem((256, 256), BF16),
        vmem((128, 256), BF16),
        vmem((32, 128), BF16),
        vmem((N, N, 256), BF16),
        vmem((N, 128), F32),
        vmem((N, N, 128), F32),
        vmem((N, N, 512), BF16),
        vmem((N, N, 512), BF16),
        vmem((N * 128, 128), BF16),
        vmem((CACHE, 128), F32),
        vmem((N, 256), BF16),
        vmem((8, N, 256), BF16),
        vmem((2, 128), F32),
        vmem((N, 2, 128), F32),
        vmem((2, 4, N, 256), BF16),
        vmem((8, N, 256), BF16),
        vmem((1, 128), F32),
        vmem((N, 1, 128), F32),
        vmem((2, 128), F32),
        vmem((N, 2, 128), F32),
        vmem((N, 256), BF16),
        vmem((N, N, 256), BF16),
        vmem((2, 128), F32),
        vmem((N, 2, 128), F32),
        vmem((32, 128), F32),
        vmem((64, 256), BF16),
        vmem((64, 256), BF16),
        vmem((8, N, 256), BF16),
        vmem((8, 80, 256), BF16),
        vmem((8, 80, 256), BF16),
        vmem((64, 128), BF16),
        vmem((N, 128), BF16),
        vmem((2, 64, 1024), BF16),
        vmem((N, N, 128), BF16),
        vmem((N, N, 256), BF16),
        vmem((N, N, 256), BF16),
        vmem((2, 128), F32),
        vmem((N, 2, 128), F32),
        vmem((64, 256), BF16),
        vmem((256, 64), BF16),
        vmem((256, 1), F32),
        pltpu.SemaphoreType.DMA((len(LOCALS),)),
        pltpu.SemaphoreType.DMA((PHASES,)),
        pltpu.SemaphoreType.DMA((PHASES,)),
        pltpu.SemaphoreType.REGULAR,
    ]
    return pl.pallas_call(
        kernel,
        out_shape=jax.ShapeDtypeStruct((N, 256), BF16),
        in_specs=[anywhere] * 21,
        out_specs=pl.BlockSpec(memory_space=pltpu.VMEM),
        scratch_shapes=scratch,
        compiler_params=pltpu.CompilerParams(
            collective_id=0, has_side_effects=True, vmem_limit_bytes=67_043_328
        ),
        name="layer",
    )(
        tokens,
        query_weight,
        key_weight,
        value_weight,
        out_weight,
        head_lambda.reshape(1, 2),
        head_gain.reshape(1, 128),
        key_cache.reshape(N, CACHE, 128),
        value_cache.reshape(N, CACHE, 128),
        lengths.reshape(1, N),
        first_gain.reshape(32, 128),
        second_gain.reshape(2, 128),
        expert_ids.T,
        route_weights.T,
        expert_gate.reshape(256, 2048),
        expert_up.reshape(256, 2048),
        expert_down.reshape(2048, 256),
        dense_gate,
        dense_up,
        dense_down,
        dense_mix.reshape(32, 128),
    )


def solution(mesh):
    return jax.shard_map(
        on_device,
        mesh=mesh,
        in_specs=(
            P("ep", None),
            P("ep", "tp"),
            P("ep", "tp"),
            P("ep", "tp"),
            P("tp", "ep"),
            P("tp"),
            P(),
            P("ep", None, "tp", None),
            P("ep", None, "tp", None),
            P("ep"),
            P(),
            P("tp"),
            P("ep", None),
            P("ep", None),
            P("ep", "tp", None),
            P("ep", "tp", None),
            P("ep", None, "tp"),
            P("tp", "ep"),
            P("tp", "ep"),
            P("ep", "tp"),
            P(),
        ),
        out_specs=P("ep", "tp"),
        check_vma=False,
    )
```

```python
import functools
import math

import jax
import jax.numpy as jnp
from jax import lax
from jax.experimental import pallas as pl
from jax.experimental.pallas import tpu as pltpu
from jax.sharding import PartitionSpec as P

N = 16
CACHE = 1024
CAP = 4
F32 = jnp.float32
BF16 = jnp.bfloat16
MESH = pl.DeviceIdType.MESH

(
    PA, PMETA, PB, PV, PW1, PW2, PWGU, PWD, PD, PE, PMEAN, PF, PG, PS, PX, PXR, PH, PI, PID, PC, PCD, PJ, PK,
) = range(23)
PHASES = 23

LOCALS = (
    "tok", "qw", "kw", "vw", "ow", "lam", "hgain", "kc", "vc", "lens", "fgain",
    "sgain", "ids", "rw", "eg", "eu", "ed", "dg", "du", "dd", "dmix",
)


def dot(a, b):
    return jnp.dot(a, b, preferred_element_type=F32)


def to_column(row, n):
    same = lax.broadcasted_iota(jnp.int32, (n, n), 0) == lax.broadcasted_iota(jnp.int32, (n, n), 1)
    return jnp.sum(jnp.where(same, jnp.broadcast_to(row, (n, n)), 0), axis=1, keepdims=True)


def to_row(column, n, lanes):
    same = lax.broadcasted_iota(jnp.int32, (n, lanes), 0) == lax.broadcasted_iota(
        jnp.int32, (n, lanes), 1
    )
    return jnp.sum(jnp.where(same, jnp.broadcast_to(column, (n, lanes)), 0), axis=0, keepdims=True)


def slot_of(i):
    return lax.rem(i, 2) * 8 + i // 2


def kernel(
    tok_h, qw_h, kw_h, vw_h, ow_h, lam_h, hgain_h, kc_h, vc_h, lens_h, fgain_h, sgain_h,
    ids_h, rw_h, eg_h, eu_h, ed_h, dg_h, du_h, dd_h, dmix_h,
    out_ref,
    tok, wqkv, wown, wo, lam, hgain, kc, vc, lens, fgain, sgain, ids, rw, wgu, wgu2, ed, wd, wd2, dd, dmix,
    xcol, meta, metas, bsend, brecv, qd, scores, normed, dnorm, vsend, vrecv, esend, erecv,
    asend, arecv, fsend, frecv, gsend, grecv, ssend, srecv, gw, xsend, xrecv, xrows,
    hsend, hrecv, isend, idsend, ihid, idense,
    jsend, jrecv, ksend, krecv, pick, place, gates,
    lsem, ssem, rsem, ready,
):
    e = lax.axis_index("ep")
    t = lax.axis_index("tp")
    z, c = t // 2, lax.rem(t, 2)
    partner = (e, 2 * z + 1 - c)
    y, x = e // 4, lax.rem(e, 4)
    e_slot = slot_of(e)

    def chunk(i, width):
        return pl.ds(pl.multiple_of(i * width, width), width)

    barrier = pltpu.get_barrier_semaphore()

    def greet(k, _):
        pl.semaphore_signal(
            barrier, inc=1, device_id=(lax.rem(e + k, N), t), device_id_type=MESH
        )
        pl.semaphore_signal(
            barrier, inc=1, device_id=(e, lax.rem(t + k, N)), device_id_type=MESH
        )
        return 0

    lax.fori_loop(1, N, greet, 0)

    coming, flights = {}, []

    def bring(name, pairs, whole=None):
        sem = lsem.at[LOCALS.index(name)]
        coming[name] = pairs[0][1] if whole is None else whole
        for src, dst in pairs:
            pltpu.make_async_copy(src, dst, sem).start()

    def arrived(name):
        whole = coming.pop(name)
        pltpu.make_async_copy(whole, whole, lsem.at[LOCALS.index(name)]).wait()

    bring("tok", [(tok_h, tok)])
    bring("ids", [(ids_h, ids)])
    bring("rw", [(rw_h, rw)])
    bring("ow", [(ow_h, wown)])
    bring("qw", [(qw_h, wqkv.at[:, 0:256])])
    bring("kw", [(kw_h, wqkv.at[:, 256:384])])
    bring("vw", [(vw_h, wqkv.at[:, 384:512])])
    bring("lens", [(lens_h, lens)])
    bring("lam", [(lam_h, lam)])
    bring("hgain", [(hgain_h, hgain)])
    bring("fgain", [(fgain_h, fgain)])
    bring("dmix", [(dmix_h, dmix)])
    bring("sgain", [(sgain_h, sgain)])

    def bring_pair(i, _):
        sem_g = lsem.at[LOCALS.index("eg")]
        sem_u = lsem.at[LOCALS.index("eu")]
        core, chip = lax.rem(i, 2), i // 2
        even = pl.ds(pl.multiple_of(chip * 256, 256), 128)
        odd = pl.ds(pl.multiple_of(chip * 256 + 128, 128), 128)
        pltpu.make_async_copy(eg_h.at[:, chunk(i, 128)], wgu.at[core, :, even], sem_g).start()
        pltpu.make_async_copy(eu_h.at[:, chunk(i, 128)], wgu.at[core, :, odd], sem_u).start()
        return 0

    lax.fori_loop(0, N, bring_pair, 0)
    coming["eg"] = wgu.at[0]
    coming["eu"] = wgu.at[1]
    bring("dg", [(dg_h, wd.at[:, 0:128])])
    bring("du", [(du_h, wd.at[:, 128:256])])
    bring("kc", [(kc_h.at[s], kc.at[:, s * 128 : (s + 1) * 128]) for s in range(N)], kc)
    bring("vc", [(vc_h.at[s], vc.at[:, s * 128 : (s + 1) * 128]) for s in range(N)], vc)

    def bring_down(i, _):
        core, chip = lax.rem(i, 2), i // 2
        pltpu.make_async_copy(
            ed_h.at[chunk(i, 128), :], ed.at[core, chunk(chip, 128), :], lsem.at[LOCALS.index("ed")]
        ).start()
        return 0

    lax.fori_loop(0, N, bring_down, 0)
    coming["ed"] = ed
    bring("dd", [(dd_h, dd)])

    def send(phase, src, dst, to):
        pltpu.make_async_remote_copy(
            src_ref=src,
            dst_ref=dst,
            send_sem=ssem.at[phase],
            recv_sem=rsem.at[phase],
            device_id=to,
            device_id_type=MESH,
        ).start()

    def far_first(i, n):
        half = (i + 1) // 2
        return n // 2 + half * (2 * lax.rem(i + 1, 2) - 1)

    def over_ep(phase, src_of, dst):
        def one(i, _):
            dy, dx = far_first(i // 4, 4), far_first(lax.rem(i, 4), 4)
            a = 4 * lax.rem(y + dy, 4) + lax.rem(x + dx, 4)
            send(phase, src_of(a), dst, (a, t))
            return 0

        lax.fori_loop(0, N - 1, one, 0)

    def over_tp(phase, src_of, dst):
        def one(i, _):
            b = lax.rem(t + far_first(i, N), N)
            send(phase, src_of(b), dst, (e, b))
            return 0

        lax.fori_loop(0, N - 1, one, 0)

    def over_z(phase, src_of, dst):
        def one(i, _):
            chip = lax.rem(z + far_first(i, 8), 8)
            send(phase, src_of(chip), dst, (e, 2 * chip + c))
            return 0

        lax.fori_loop(0, 7, one, 0)

    def received(phase, blocks):
        pltpu.make_async_copy(blocks, blocks, rsem.at[phase]).wait()

    def sent(phase, blocks):
        pltpu.make_async_copy(blocks, blocks, ssem.at[phase]).wait()

    lane = lax.broadcasted_iota(jnp.int32, (N, 128), 1)

    arrived("ids")
    arrived("rw")
    id0 = to_column(ids[0:1, :], N)
    id1 = to_column(ids[1:2, :], N)
    w0 = to_column(rw[0:1, :], N)
    w1 = to_column(rw[1:2, :], N)
    total = w0 + w1
    hit0 = lane == id0
    hit1 = lane == id1
    hit = jnp.where(hit0 | hit1, 1.0, 0.0).astype(F32)
    before = jnp.where(
        lax.broadcasted_iota(jnp.int32, (N, N), 1) < lax.broadcasted_iota(jnp.int32, (N, N), 0),
        1.0,
        0.0,
    ).astype(F32)
    slot = dot(before.astype(BF16), hit.astype(BF16))
    code = jnp.where(hit > 0.5, slot, -1.0)
    gate0 = jnp.where(lane - N == id0, w0 / total, 0.0)
    gate1 = jnp.where(lane - N == id1, w1 / total, 0.0)
    meta[...] = jnp.where(lane < N, code, gate0 + gate1)
    metas[e_slot] = meta[...]

    arrived("lens")
    length = to_column(lens[...], N)
    turn = lax.rem(lane, 32).astype(F32) * (2.0 / 64)
    angle = length.astype(F32) * jnp.exp(turn * (-math.log(500000.0)))
    low = lax.rem(lane, 64) < 32
    cosine = jnp.cos(angle)
    sine = jnp.sin(angle)
    sine = jnp.where(low, -sine, sine)

    arrived("tok")
    xcol[e] = tok[:, chunk(e, 256)]
    arrived("ow")
    heads_sum = to_row(jnp.sum(wown[...].astype(F32), axis=1, keepdims=True), 256, 256)
    vsend[0:1, :] = heads_sum[:, 0:128]
    vsend[1:2, :] = heads_sum[:, 128:256]
    vrecv[e] = vsend[...]

    pl.semaphore_wait(barrier, 2 * (N - 1))

    over_ep(PA, lambda a: tok.at[:, chunk(a, 256)], xcol.at[e])
    flights.append((PA, xcol.at[0:15]))

    def tell(k, _):
        pl.semaphore_signal(ready, inc=1, device_id=(e, lax.rem(t + k, N)), device_id_type=MESH)
        return 0

    lax.fori_loop(1, N, tell, 0)

    arrived("qw")
    arrived("kw")
    arrived("vw")
    received(PA, xcol.at[0:15])
    bsend[...] = dot(xcol[...].reshape(256, 256), wqkv[...]).astype(BF16).reshape(N, N, 512)
    brecv[e] = bsend[e]
    over_ep(PB, lambda a: bsend.at[a], brecv.at[e])
    flights.append((PB, bsend.at[0:15]))

    after, ahead = 4 * y + lax.rem(x + 1, 4), 4 * y + lax.rem(x + 3, 4)
    goal = lax.rem(x, 2)
    same = goal == c
    other = jnp.logical_not(same)
    landing = wo.at[x // 2, chunk(c, 256)]
    send(PW1, wown, landing, (after, 2 * z + goal))
    send(PW1, wown, landing, (ahead, 2 * z + goal))

    @pl.when(same)
    def _():
        pltpu.make_async_copy(wown, landing, rsem.at[PW1]).start()

    @pl.when(other)
    def _():
        send(PW1, wown, landing, partner)

    flights.append((PW1, wo.at[0]))
    over_ep(PV, lambda a: vsend, vrecv.at[e])
    flights.append((PV, vrecv.at[0:15]))

    received(PB, brecv.at[0:15])
    arrived("eg")
    arrived("eu")
    arrived("dg")
    arrived("du")
    send(PWGU, wgu.at[1 - c], wgu2, partner)
    flights.append((PWGU, wgu2))
    send(PWD, wd, wd2, partner)
    flights.append((PWD, wd2))

    qkv = jnp.sum(brecv[...].astype(F32), axis=0).astype(BF16).astype(F32)

    def rotated(v):
        swapped = jnp.where(low, pltpu.roll(v, 96, 1), pltpu.roll(v, 32, 1))
        return (v * cosine + swapped * sine).astype(BF16).astype(F32)

    first = lane < 64
    key = rotated(qkv[:, 256:384])
    value = qkv[:, 384:512]
    parts, fresh = [], jnp.zeros((1, 128), F32)
    seq = lax.broadcasted_iota(jnp.int32, (N, 128), 0)
    for sub in range(2):
        for g in range(2):
            q = rotated(qkv[:, g * 128 : (g + 1) * 128]) * 0.125
            q = jnp.where(first if sub == 0 else jnp.logical_not(first), q, 0.0)
            score = jnp.sum(q * key, axis=1, keepdims=True)
            at = lane == (2 * sub + g) * N + seq
            fresh = fresh + jnp.sum(jnp.where(at, score, 0.0), axis=0, keepdims=True)
            parts.append(q)
    turned = jnp.concatenate(parts + [jnp.zeros((64, 128), F32)], axis=0).T
    lane128 = lax.broadcasted_iota(jnp.int32, (128, 128), 1)
    for s in range(N):
        keep = (lax.rem(lane128, N) == s) & (lane128 < 64)
        qd[s * 128 : (s + 1) * 128, :] = jnp.where(keep, turned, 0.0).astype(BF16)

    arrived("lam")
    row = lax.broadcasted_iota(jnp.int32, (1, 128), 1)
    share = jnp.where(
        row < 2 * N, 1.0, jnp.where(row < 3 * N, -lam[0:1, 0:1], -lam[0:1, 1:2])
    )
    limit = jnp.sum(jnp.where(lax.rem(lane, N) == seq, length, 0), axis=0, keepdims=True)

    arrived("kc")
    scores[...] = dot(kc[...], qd[...])
    position = lax.broadcasted_iota(jnp.int32, (CACHE, 128), 0)
    masked = jnp.where(position < limit, scores[...], -1e30)
    top = jnp.maximum(jnp.max(masked, axis=0, keepdims=True), fresh)
    p = jnp.exp(masked - top)
    fresh_p = jnp.exp(fresh - top)
    scale = share / (jnp.sum(p, axis=0, keepdims=True) + fresh_p)
    p = p * scale
    fresh_p = fresh_p * scale
    p = p + pltpu.roll(p, 96, 1)
    fresh_p = jnp.broadcast_to(fresh_p, (8, 128))
    fresh_p = (fresh_p + pltpu.roll(fresh_p, 96, 1)).astype(BF16).astype(F32)[0:1, :]
    chances = p.T[0 : 2 * N, :].astype(BF16)
    arrived("vc")
    @pl.when(same)
    def _():
        received(PW1, wo.at[0])

    @pl.when(other)
    def _():
        received(PW1, wo)
        x_up, x_down = lax.rem(x + 3, 4), lax.rem(x + 1, 4)
        low_half, high_half = wo.at[x_down // 2, 0:256], wo.at[x_up // 2, 256:512]
        send(PW2, low_half, low_half, (ahead, t))
        send(PW2, high_half, high_half, (after, t))

    heads = dot(chances, vc[...])

    arrived("hgain")
    for g in range(2):
        weight = jnp.sum(jnp.where(lane == g * N + seq, fresh_p, 0.0), axis=1, keepdims=True)
        head = weight * value
        for s in range(N):
            head = head + jnp.where(
                seq == s, heads[g * N : (g + 1) * N, s * 128 : (s + 1) * 128], 0.0
            )
        mean = jnp.mean(head * head, axis=1, keepdims=True)
        head = head * lax.rsqrt(mean + 1e-6) * hgain[...] * 0.8
        normed[:, g * 128 : (g + 1) * 128] = head.astype(BF16)
    pl.semaphore_wait(ready, N - 1)
    dnorm[c * 4 + y] = normed[...]

    def heads_send(k, _):
        e2 = 4 * lax.rem(y + k, 4) + x
        send(PD, normed, dnorm.at[c * 4 + y], (e2, t))
        send(PD, normed, dnorm.at[c * 4 + y], (e2, 2 * z + 1 - c))
        return 0

    lax.fori_loop(1, 4, heads_send, 0)
    send(PD, normed, dnorm.at[c * 4 + y], partner)
    flights.append((PD, dnorm.at[0:7]))
    received(PV, vrecv.at[0:15])
    weights_sum = jnp.sum(vrecv[...], axis=0)
    sums = jnp.sum(
        normed[:, 0:128].astype(F32) * weights_sum[0:1, :]
        + normed[:, 128:256].astype(F32) * weights_sum[1:2, :],
        axis=1,
        keepdims=True,
    )
    asend[...] = to_row(sums, N, 128)
    arecv[t] = asend[...]
    over_tp(PMEAN, lambda b: asend, arecv.at[t])
    flights.append((PMEAN, arecv.at[0:15]))

    @pl.when(same)
    def _():
        received(PW2, wo.at[0])

    received(PD, dnorm.at[0:7])

    def out_send(i, _):
        j, y2 = i // 4, lax.rem(y + 2 + lax.rem(i, 4), 4)
        b = 4 * y + 2 * j + c
        itself = (y2 == y) & (b == t)

        @pl.when(lax.rem(i, 4) == 0)
        def _():
            part = dot(dnorm[0:4].reshape(64, 256), wo[j, 0:256])
            part = part + dot(dnorm[4:8].reshape(64, 256), wo[j, 256:512])
            esend[j] = part.astype(BF16).reshape(4, N, 256)

        @pl.when(itself)
        def _():
            pltpu.make_async_copy(esend.at[j, y2], erecv.at[z], rsem.at[PE]).start()

        @pl.when(jnp.logical_not(itself))
        def _():
            send(PE, esend.at[j, y2], erecv.at[z], (4 * y2 + x, b))

        return 0

    lax.fori_loop(0, 8, out_send, 0)
    flights.append((PE, erecv.at[0:7]))
    over_ep(PMETA, lambda a: meta, metas.at[e_slot])
    flights.append((PMETA, metas.at[0:15]))

    received(PMETA, metas.at[0:15])
    every = metas[...].reshape(256, 128)
    wide_lane = lax.broadcasted_iota(jnp.int32, (256, 128), 1)
    code_col = jnp.sum(jnp.where(wide_lane == e, every, 0.0), axis=1, keepdims=True)
    gate_col = jnp.sum(jnp.where(wide_lane == e + N, every, 0.0), axis=1, keepdims=True)
    block = (lax.broadcasted_iota(jnp.int32, (256, 1), 0) // N * CAP).astype(F32)
    target = jnp.where(code_col >= 0.0, code_col + block, -1.0)
    place[...] = jnp.where(
        lax.broadcasted_iota(jnp.int32, (256, 64), 1).astype(F32) == target, 1.0, 0.0
    ).astype(BF16)
    pick[...] = jnp.where(
        lax.broadcasted_iota(jnp.int32, (64, 256), 0).astype(F32) == to_row(target, 256, 256),
        1.0,
        0.0,
    ).astype(BF16)
    gates[...] = gate_col

    arrived("fgain")
    arrived("dmix")
    gw[...] = fgain[...] * dmix[...].astype(F32)

    def block_of(ref):
        return jnp.concatenate([ref[pl.ds(2 * t, 1), :], ref[pl.ds(2 * t + 1, 1), :]], axis=1)

    gain = block_of(fgain)
    gain_mix = block_of(gw)
    root = 2.0**0.5
    token_mean = root * jnp.mean(tok[...].astype(F32), axis=1, keepdims=True)
    own_tokens = root * tok[:, chunk(t, 256)].astype(F32)

    received(PE, erecv)
    residual = own_tokens + jnp.sum(erecv[...].astype(F32), axis=0)
    received(PMEAN, arecv.at[0:15])
    mean = token_mean + to_column_of(jnp.sum(arecv[...], axis=0)) * (1.0 / 4096)
    centred = residual - mean
    gsend[...] = (centred * gain).astype(BF16)
    grecv[e_slot] = gsend[...]
    over_ep(PG, lambda a: gsend, grecv.at[e_slot])
    flights.append((PG, grecv.at[0:15]))
    fsend[0:1, :] = to_row(jnp.sum(centred * centred, axis=1, keepdims=True), N, 128)
    fsend[1:2, :] = to_row(jnp.sum(centred * gain_mix, axis=1, keepdims=True), N, 128)
    frecv[t] = fsend[...]
    over_tp(PF, lambda b: fsend, frecv.at[t])
    flights.append((PF, frecv.at[0:15]))

    received(PG, grecv.at[0:15])
    xsend[...] = dot(pick[...], grecv[...].reshape(256, 256)).astype(BF16)
    send(PX, xsend, xrecv, partner)
    flights.append((PX, xrecv))
    send(PXR, grecv.at[pl.ds((1 - c) * 8, 8)], xrows, partner)
    flights.append((PXR, xrows))

    received(PWGU, wgu2)
    received(PWD, wd2)
    received(PX, xrecv)
    received(PXR, xrows)
    mine = grecv[pl.ds(c * 8, 8)].reshape(128, 256)
    dense_pre = dot(mine, wd[...]) + dot(xrows[...].reshape(128, 256), wd2[...])
    hsend[:, 64:80, :] = dense_pre.astype(BF16).reshape(8, N, 256)

    def partial(chip):
        cols = chunk(chip, 256)
        pre = dot(xsend[...], wgu[c, :, cols]) + dot(xrecv[...], wgu2[:, cols])
        hsend[chip, 0:64, :] = pre.astype(BF16)

    def project(i, _):
        chip = lax.rem(z + far_first(i, 8), 8)
        partial(chip)
        send(PH, hsend.at[chip], hrecv.at[z], (e, 2 * chip + c))
        return 0

    lax.fori_loop(0, 7, project, 0)
    flights.append((PH, hsend.at[0:7]))
    partial(z)
    hrecv[z] = hsend[z]

    received(PF, frecv.at[0:15])
    totals = jnp.sum(frecv[...], axis=0)
    scale_row = lax.rsqrt(totals[0:1, :] * (1.0 / 4096) + 1e-5)
    mix = 1.0 / (1.0 + jnp.exp(-scale_row * totals[1:2, :]))
    ssend[0:1, :] = scale_row
    ssend[1:2, :] = mix
    srecv[e_slot] = ssend[...]
    over_ep(PS, lambda a: ssend, srecv.at[e_slot])
    flights.append((PS, srecv.at[0:15]))

    received(PS, srecv.at[0:15])
    own = lax.broadcasted_iota(jnp.int32, (N, N, 128), 1) == lax.broadcasted_iota(
        jnp.int32, (N, N, 128), 2
    )

    def token_column(rows):
        spread = jnp.where(own, jnp.broadcast_to(rows, (N, N, 128)), 0.0)
        return jnp.sum(spread, axis=2, keepdims=True).reshape(256, 1)

    mix_col = token_column(srecv[:, 1:2, :])
    scale_col = token_column(srecv[:, 0:1, :])
    row_scale = to_column(
        jnp.sum(jnp.where(place[...].astype(F32) > 0.5, scale_col, 0.0), axis=0, keepdims=True), 64
    )
    dense_scale = to_column_of(srecv[slot_of(t), 0:1, :])
    all_scale = jnp.concatenate([row_scale, dense_scale], axis=0)
    hidden = centred * to_column_of(scale_row) * gain

    received(PH, hrecv.at[0:7])
    pre = jnp.sum(hrecv[...].astype(F32), axis=0) * all_scale
    pre_gate = pre[:, 0:128]
    active = (pre_gate / (1.0 + jnp.exp(-pre_gate)) * pre[:, 128:256]).astype(BF16)
    isend[...] = active[0:64, :]
    idsend[...] = active[64:80, :]
    ihid[c, :, chunk(z, 128)] = isend[...]
    idense[c * 8 + z] = idsend[...]
    over_z(PI, lambda chip: isend, ihid.at[c, :, chunk(z, 128)])
    flights.append((PI, ihid.at[0, :, 0 : 7 * 128]))
    over_z(PID, lambda chip: idsend, idense.at[c * 8 + z])
    flights.append((PID, idense.at[0:7]))
    arrived("ed")
    arrived("dd")
    received(PI, ihid.at[0, :, 0 : 7 * 128])
    send(PC, ihid.at[c], ihid.at[c], partner)
    flights.append((PC, ihid.at[0]))
    received(PID, idense.at[0:7])
    send(PCD, idense.at[pl.ds(c * 8, 8)], idense.at[pl.ds(c * 8, 8)], partner)
    flights.append((PCD, idense.at[0:8]))
    result = dot(ihid[c], ed[c])
    received(PC, ihid.at[0])
    received(PCD, idense.at[0:8])
    result = (result + dot(ihid[1 - c], ed[1 - c])).astype(BF16)
    dense = dot(idense[...].reshape(256, 128), dd[...]) * mix_col
    mixture = dot(place[...], result) * gates[...] + dense
    jsend[...] = mixture.astype(BF16).reshape(N, N, 256)
    jrecv[e] = jsend[e_slot]
    over_ep(PJ, lambda a: jsend.at[slot_of(a)], jrecv.at[e])
    flights.append((PJ, jsend.at[0:15]))
    arrived("sgain")
    received(PJ, jrecv.at[0:15])
    combined = root * hidden.astype(BF16).astype(F32) + jnp.sum(jrecv[...].astype(F32), axis=0)

    mean_b = jnp.sum(combined, axis=1, keepdims=True) * (1.0 / 256)
    apart = combined - mean_b
    ksend[0:1, :] = to_row(mean_b, N, 128)
    ksend[1:2, :] = to_row(jnp.sum(apart * apart, axis=1, keepdims=True), N, 128)
    krecv[t] = ksend[...]
    over_tp(PK, lambda b: ksend, krecv.at[t])
    flights.append((PK, krecv.at[0:15]))
    received(PK, krecv.at[0:15])
    means = krecv[:, 0, :]
    mean = jnp.sum(means, axis=0, keepdims=True) * (1.0 / N)
    off = means - mean
    square = jnp.sum(krecv[:, 1, :] + 256.0 * off * off, axis=0, keepdims=True)
    scale = lax.rsqrt(square * (1.0 / 4096) + 1e-5)
    last_gain = jnp.concatenate([sgain[0:1, :], sgain[1:2, :]], axis=1)
    out_ref[...] = (
        (combined - to_column_of(mean)) * to_column_of(scale) * last_gain
    ).astype(BF16)

    for phase, blocks in flights:
        sent(phase, blocks)

    @pl.when(other)
    def _():
        sent(PW1, wown)
        sent(PW2, wo.at[0])

    if any(phase == PE for phase, _ in flights):

        @pl.when(t // 4 != y)
        def _():
            sent(PE, erecv.at[0])


def to_column_of(row):
    same = lax.broadcasted_iota(jnp.int32, (N, 128), 0) == lax.broadcasted_iota(
        jnp.int32, (N, 128), 1
    )
    return jnp.sum(jnp.where(same, jnp.broadcast_to(row, (N, 128)), 0), axis=1, keepdims=True)


def on_device(
    tokens, query_weight, key_weight, value_weight, out_weight, head_lambda, head_gain,
    key_cache, value_cache, lengths, first_gain, second_gain, expert_ids, route_weights,
    expert_gate, expert_up, expert_down, dense_gate, dense_up, dense_down, dense_mix,
):
    anywhere = pl.BlockSpec(memory_space=pltpu.HBM)
    vmem = pltpu.VMEM
    scratch = [
        vmem((N, 4096), BF16),
        vmem((256, 512), BF16),
        vmem((256, 256), BF16),
        vmem((2, 512, 256), BF16),
        vmem((1, 2), F32),
        vmem((1, 128), F32),
        vmem((CACHE, N * 128), BF16),
        vmem((CACHE, N * 128), BF16),
        vmem((1, N), jnp.int32),
        vmem((32, 128), F32),
        vmem((2, 128), F32),
        vmem((2, N), jnp.int32),
        vmem((2, N), F32),
        vmem((2, 256, 2048), BF16),
        vmem((256, 2048), BF16),
        vmem((2, 1024, 256), BF16),
        vmem((256, 256), BF16),
        vmem((256, 256), BF16),
        vmem((128, 256), BF16),
        vmem((32, 128), BF16),
        vmem((N, N, 256), BF16),
        vmem((N, 128), F32),
        vmem((N, N, 128), F32),
        vmem((N, N, 512), BF16),
        vmem((N, N, 512), BF16),
        vmem((N * 128, 128), BF16),
        vmem((CACHE, 128), F32),
        vmem((N, 256), BF16),
        vmem((8, N, 256), BF16),
        vmem((2, 128), F32),
        vmem((N, 2, 128), F32),
        vmem((2, 4, N, 256), BF16),
        vmem((8, N, 256), BF16),
        vmem((1, 128), F32),
        vmem((N, 1, 128), F32),
        vmem((2, 128), F32),
        vmem((N, 2, 128), F32),
        vmem((N, 256), BF16),
        vmem((N, N, 256), BF16),
        vmem((2, 128), F32),
        vmem((N, 2, 128), F32),
        vmem((32, 128), F32),
        vmem((64, 256), BF16),
        vmem((64, 256), BF16),
        vmem((8, N, 256), BF16),
        vmem((8, 80, 256), BF16),
        vmem((8, 80, 256), BF16),
        vmem((64, 128), BF16),
        vmem((N, 128), BF16),
        vmem((2, 64, 1024), BF16),
        vmem((N, N, 128), BF16),
        vmem((N, N, 256), BF16),
        vmem((N, N, 256), BF16),
        vmem((2, 128), F32),
        vmem((N, 2, 128), F32),
        vmem((64, 256), BF16),
        vmem((256, 64), BF16),
        vmem((256, 1), F32),
        pltpu.SemaphoreType.DMA((len(LOCALS),)),
        pltpu.SemaphoreType.DMA((PHASES,)),
        pltpu.SemaphoreType.DMA((PHASES,)),
        pltpu.SemaphoreType.REGULAR,
    ]
    return pl.pallas_call(
        kernel,
        out_shape=jax.ShapeDtypeStruct((N, 256), BF16),
        in_specs=[anywhere] * 21,
        out_specs=pl.BlockSpec(memory_space=pltpu.VMEM),
        scratch_shapes=scratch,
        compiler_params=pltpu.CompilerParams(
            collective_id=0, has_side_effects=True, vmem_limit_bytes=67_043_328
        ),
        name="layer",
    )(
        tokens,
        query_weight,
        key_weight,
        value_weight,
        out_weight,
        head_lambda.reshape(1, 2),
        head_gain.reshape(1, 128),
        key_cache.reshape(N, CACHE, 128),
        value_cache.reshape(N, CACHE, 128),
        lengths.reshape(1, N),
        first_gain.reshape(32, 128),
        second_gain.reshape(2, 128),
        expert_ids.T,
        route_weights.T,
        expert_gate.reshape(256, 2048),
        expert_up.reshape(256, 2048),
        expert_down.reshape(2048, 256),
        dense_gate,
        dense_up,
        dense_down,
        dense_mix.reshape(32, 128),
    )


def solution(mesh):
    return jax.shard_map(
        on_device,
        mesh=mesh,
        in_specs=(
            P("ep", None),
            P("ep", "tp"),
            P("ep", "tp"),
            P("ep", "tp"),
            P("tp", "ep"),
            P("tp"),
            P(),
            P("ep", None, "tp", None),
            P("ep", None, "tp", None),
            P("ep"),
            P(),
            P("tp"),
            P("ep", None),
            P("ep", None),
            P("ep", "tp", None),
            P("ep", "tp", None),
            P("ep", None, "tp"),
            P("tp", "ep"),
            P("tp", "ep"),
            P("ep", "tp"),
            P(),
        ),
        out_specs=P("ep", "tp"),
        check_vma=False,
    )
```
